32 devices in a mesh: sp: 8 (over z, core), tp: 4 (over y, x).
Axes of the slice: x: 2, y: 2, z: 4, core: 2. Of those that a mesh axis runs over, the one named last changes fastest.
Arguments:
- moe_input: bfloat16 [1024, 2048], P('sp', 'tp'), may hold values from -6 to 6
- cotangent: bfloat16 [1024, 2048], P('sp', 'tp'), may hold values from -6 to 6
- routes: int32 [1024, 2], P('sp'), may hold values from 0 to 7, all different within a row; in each aligned block of 128 rows (0 to 127, 128 to 255, ...) at most 64 rows name the same one
- route_weight: float32 [1024, 2], P('sp'), may hold values from 0.1 to 1
- w_gate: bfloat16 [8, 2816, 2048], P('sp', 'tp'), may hold values from -0.125 to 0.125
- w_up: bfloat16 [8, 2816, 2048], P('sp', 'tp'), may hold values from -0.125 to 0.125
- w_down: bfloat16 [8, 2816, 2048], P('sp', 'tp'), may hold values from -0.109375 to 0.109375
- v_value: bfloat16 [1024, 1024], P('sp', 'tp'), may hold values from -6 to 6
- v_gate: bfloat16 [1024, 1024], P('sp', 'tp'), may hold values from -12 to 12
- conv_out: bfloat16 [1024, 1024], P('sp', 'tp'), may hold values from -6 to 6
- row_mean: float32 [1024], P('sp'), may hold values from -3 to 3
- row_rstd: float32 [1024], P('sp'), may hold values from 0.5 to 2
- ln_gain: float32 [1024], P('tp'), may hold values from 0.1 to 1.9
- taps: bfloat16 [31, 1024], P(None, 'tp'), may hold values from -1 to 1
- out_proj: bfloat16 [2048, 1024], P('sp', 'tp'), may hold values from -0.1875 to 0.1875
Outputs:
- gate_grad: bfloat16 [8, 2816, 2048], P('sp', 'tp')
- up_grad: bfloat16 [8, 2816, 2048], P('sp', 'tp')
- down_grad: bfloat16 [8, 2816, 2048], P('sp', 'tp')
- proj_grad: float32 [2048, 1024], P('sp', 'tp')
- stream_grad: bfloat16 [1024, 2048], P('sp', 'tp')
- value_grad: bfloat16 [1024, 1024], P('sp', 'tp')
- gating_grad: bfloat16 [1024, 1024], P('sp', 'tp')
The draws below stay inside these ranges and needn't reach their ends.
Inputs may be any that keep to these rules, and one draw needn't show every extreme that they name: `routes`: in the rows of one device no expert is named more than 64 times.
All inputs are finite; a program needn't handle non-finite values.
Results may differ from the reference program's by a relative error of at most 0.025.
Values may be sent and summed in bfloat16 or wider, within the bound.
A program may use at most 64 MiB of HBM per device.

```python
import math
import jax
import jax.numpy as jnp
import numpy as np
from jax import lax

D = 2048
FF = 2816
CW = 1024
KERNEL = 31
TOK_DEV = 128
TOKENS = 1024
EXPERTS = 8
CAP = 64
N_SP = 8
N_TP = 4


def spiked(values, key, source, target, shards_of, factor):
    def block_of(axis_at):
        return (jnp.arange(values.shape[axis_at]) // (values.shape[axis_at] // shards_of)).reshape((-1,) + (1,) * (values.ndim - 1 - axis_at))

    first = jax.random.permutation(key, shards_of)[block_of(target)]
    other_side = (block_of(target) + shards_of // 2) % shards_of
    return jnp.where((block_of(source) == first) | (block_of(source) == other_side), factor * values, values)


def shard_levels(rng, extent, split, least, top_value):
    loudness = 1.0
    for dim, shards_of in split:
        draws = jax.random.uniform(jax.random.fold_in(jax.random.fold_in(rng, 6), dim), (shards_of,), jnp.float32, least / len(split), top_value / len(split))
        loudness = loudness * jnp.repeat(jnp.exp(draws), extent[dim] // shards_of).reshape((-1,) + (1,) * (len(extent) - 1 - dim))
    return loudness


def routed_block(rng, own, number, rows, number_of, top, bound, lean):
    sequence = jax.random.permutation(rng, number_of)
    crowded, usual = portions_of(number_of, rows * top, bound, lean, True), portions_of(number_of, rows * top, bound, lean, False)
    places = jnp.arange(number_of)

    def named(sizes, offset_by):
        used = int((sizes > 0).sum())
        fixed = max(1, used // 4)
        passed = fixed + (places - fixed + offset_by * (used - fixed)) % max(1, number_of - fixed)
        return jnp.zeros((number_of,), jnp.int32).at[sequence[jnp.where(places < fixed, places, passed)]].set(jnp.asarray(sizes, jnp.int32))

    sizes = jnp.where(number % 4 == 0, named(crowded, number // 4), named(usual, number - number // 4 - 1))
    mixed = jax.random.permutation(jax.random.fold_in(own, 3), number_of)
    source_of, receiver = mixed[0:number_of // 2 * 2:2], mixed[1:number_of // 2 * 2:2]
    slack = jnp.minimum(sizes[source_of] - 1, bound - sizes[receiver]) // 2
    slack = jnp.where((source_of == sequence[0]) | (receiver == sequence[0]) | (sizes[receiver] == 0), 0, jnp.maximum(slack, 0))
    passed = jax.random.randint(jax.random.fold_in(own, 4), (number_of // 2,), 0, 1 << 20) % (slack + 1)
    sizes = sizes.at[source_of].add(-passed).at[receiver].add(passed)
    members = jnp.searchsorted(jnp.cumsum(sizes), jnp.arange(rows * top), side="right").astype(jnp.int32)
    table = members.reshape(top, rows).T
    table = table[jax.random.permutation(jax.random.fold_in(own, 1), rows)]
    offset_by = jax.random.randint(jax.random.fold_in(own, 2), (rows, 1), 0, top)
    return jnp.take_along_axis(table, (jnp.arange(top)[None, :] + offset_by) % top, axis=1)


def portions_of(number_of, total, reach, lean, full):
    portions = [(1 << 20) // math.isqrt(standing ** lean) + 1 for standing in range(1, number_of + 1)]
    largest = reach if full else min(reach, max(-(-total // number_of), total * portions[0] // sum(portions)))
    least = 1 if total - largest >= number_of - 1 else 0
    holding, rest = [largest] + [least] * (number_of - 1), total - largest - least * (number_of - 1)
    while rest > 0:
        movable = [i for i in range(1, number_of) if holding[i] < largest] or [i for i in range(1, number_of) if holding[i] < reach]
        pool, budget = sum([portions[i] for i in movable]), rest
        for i in movable:
            addition = min(reach - holding[i], max(1, budget * portions[i] // pool), rest)
            holding[i] = holding[i] + addition
            rest = rest - addition
    return np.array(holding)


def scatter_about(rng, shape, deviation, reach, shards=(), kind=jnp.bfloat16):
    array = jax.random.normal(rng, shape, jnp.float32) * deviation
    if len(shards) > 0:
        array = shard_levels(rng, shape, shards, -0.22, 0.18) * array
    return jnp.clip(array, min=-reach, max=reach).astype(kind)


def heavy_noise(stream_key, dims, deviation, most, shards, heavy, kind=jnp.bfloat16):
    values = deviation * jax.random.normal(stream_key, dims, jnp.float32)
    if shards:
        values = values * shard_levels(stream_key, dims, shards, -0.22, 0.18)
    return jnp.clip(spiked(values, jax.random.fold_in(stream_key, 3), *heavy), -most, most).astype(kind)


def setup_inputs(seed: int = 0) -> dict:
    key_list = jax.random.split(jax.random.key(seed), 16)
    moe_input = scatter_about(key_list[0], (TOKENS, D), 1.0, 6.0, ((0, 8), (1, 4)))
    cotangent = heavy_noise(key_list[1], (TOKENS, D), 1.0, 6.0, ((0, 8), (1, 4)), (0, 1, 8, 2.0))
    routes_keys = jax.random.split(jax.random.fold_in(key_list[2], 1), TOKENS // TOK_DEV)
    routes_turns = jax.random.permutation(jax.random.fold_in(key_list[2], 3), TOKENS // TOK_DEV)
    routes = jax.vmap(lambda own, number: routed_block(jax.random.fold_in(key_list[2], 2), own, number, TOK_DEV, EXPERTS, 2, CAP, 2))(routes_keys, routes_turns).reshape((TOKENS, 2))
    route_weight = jnp.clip(0.1 + 0.9 * jax.random.uniform(key_list[3], (TOKENS, 2), jnp.float32) ** shard_levels(key_list[3], (TOKENS, 2), ((0, 8),), -0.2, 0.2), 0.1, 1.0)
    w_gate = scatter_about(key_list[4], (EXPERTS, FF, D), D ** -0.5, 0.125, ((0, 8), (1, 4)))
    w_up = scatter_about(key_list[5], (EXPERTS, FF, D), D ** -0.5, 0.125, ((0, 8), (1, 4)))
    w_down = scatter_about(key_list[6], (EXPERTS, FF, D), FF ** -0.5, 0.109375, ((0, 8), (1, 4)))
    v_value = scatter_about(key_list[7], (TOKENS, CW), 1.0, 6.0, ((0, 8), (1, 4)))
    v_gate = scatter_about(key_list[8], (TOKENS, CW), 2.0, 12.0, ((0, 8), (1, 4)))
    conv_out = scatter_about(key_list[9], (TOKENS, CW), 1.0, 6.0, ((0, 8), (1, 4)))
    row_mean = scatter_about(key_list[10], (TOKENS,), 0.5, 3.0, ((0, 8),), jnp.float32)
    row_rstd = jnp.clip(jnp.exp(math.log(2.0) - 1.3862944 * jax.random.uniform(key_list[11], (TOKENS,), jnp.float32) ** shard_levels(key_list[11], (TOKENS,), ((0, 8),), -0.2, 0.2)), 0.5, 2.0)
    ln_gain = jnp.clip(1.0 + 0.18 * jax.random.normal(key_list[12], (CW,), jnp.float32), 0.1, 1.9)
    taps = scatter_about(key_list[13], (KERNEL, CW), KERNEL ** -0.5, 1.0, ((1, 4),))
    out_proj = scatter_about(key_list[14], (D, CW), CW ** -0.5, 0.1875, ((0, 8), (1, 4)))
    return {"moe_input": moe_input, "cotangent": cotangent, "routes": routes, "route_weight": route_weight, "w_gate": w_gate, "w_up": w_up, "w_down": w_down, "v_value": v_value, "v_gate": v_gate, "conv_out": conv_out, "row_mean": row_mean, "row_rstd": row_rstd, "ln_gain": ln_gain, "taps": taps, "out_proj": out_proj}


def slot_numbers(block_routes):
    member = (block_routes[:, None] == jnp.arange(N_SP, dtype=jnp.int32)[None, :]).astype(jnp.int32)
    earlier = jnp.cumsum(member, axis=0) - member
    return jnp.sum(earlier * member, axis=1).astype(jnp.int32)


def expert_pass(operands):
    rows, cotan, gate_w, up_w, down_w = operands
    total = rows.shape[0]
    gate_pre = jnp.dot(rows, gate_w.T, preferred_element_type=jnp.float32)
    up_pre = jnp.dot(rows, up_w.T, preferred_element_type=jnp.float32)
    gate_sig = jax.nn.sigmoid(gate_pre)
    gate_act = gate_pre * gate_sig
    hidden = (gate_act * up_pre).astype(jnp.bfloat16)
    down_g = jnp.dot(hidden.T, cotan, preferred_element_type=jnp.float32).astype(jnp.bfloat16)
    hidden_grad = jnp.dot(cotan, down_w.T, preferred_element_type=jnp.float32)
    gate_delta = (hidden_grad * up_pre * gate_sig * (1.0 + gate_pre * (1.0 - gate_sig))).astype(jnp.bfloat16)
    up_delta = (hidden_grad * gate_act).astype(jnp.bfloat16)
    gate_g = jnp.dot(gate_delta.T, rows, preferred_element_type=jnp.float32).astype(jnp.bfloat16)
    up_g = jnp.dot(up_delta.T, rows, preferred_element_type=jnp.float32).astype(jnp.bfloat16)
    per_block = FF // N_TP
    gate_three = gate_delta.astype(jnp.float32).reshape(total, N_TP, per_block)
    up_three = up_delta.astype(jnp.float32).reshape(total, N_TP, per_block)
    gate_wt = gate_w.astype(jnp.float32).reshape(N_TP, per_block, D)
    up_wt = up_w.astype(jnp.float32).reshape(N_TP, per_block, D)
    partial_value = jnp.einsum('rnf,nfd->nrd', gate_three, gate_wt) + jnp.einsum('rnf,nfd->nrd', up_three, up_wt)
    rounded = lax.optimization_barrier(partial_value.astype(jnp.bfloat16))
    row_g = jnp.sum(rounded.astype(jnp.float32), axis=0).astype(jnp.bfloat16)
    return gate_g, up_g, down_g, row_g


def reference(moe_input, cotangent, routes, route_weight, w_gate, w_up, w_down, v_value, v_gate,
              conv_out, row_mean, row_rstd, ln_gain, taps, out_proj):
    buffer_len = N_SP * CAP
    block_routes = routes.reshape(N_SP, 2 * TOK_DEV).astype(jnp.int32)
    slot_index = jax.vmap(slot_numbers)(block_routes)
    source = jnp.arange(N_SP, dtype=jnp.int32)[:, None]
    buffer_row = (block_routes * buffer_len + source * CAP + slot_index).reshape(-1).astype(jnp.int32)
    token_index = (jnp.arange(2 * TOKENS, dtype=jnp.int32) // 2).astype(jnp.int32)
    picked = moe_input[token_index]
    weighted = (route_weight.reshape(-1)[:, None] * cotangent[token_index].astype(jnp.float32)).astype(jnp.bfloat16)
    rows_all = jnp.zeros((EXPERTS * buffer_len, D), jnp.bfloat16).at[buffer_row].set(picked)
    cotan_all = jnp.zeros((EXPERTS * buffer_len, D), jnp.bfloat16).at[buffer_row].set(weighted)
    rows_all = rows_all.reshape(EXPERTS, buffer_len, D)
    cotan_all = cotan_all.reshape(EXPERTS, buffer_len, D)
    gate_g, up_g, down_g, row_g = lax.map(expert_pass, (rows_all, cotan_all, w_gate, w_up, w_down))
    returned = row_g.reshape(EXPERTS * buffer_len, D)[buffer_row].astype(jnp.float32)
    returned = returned.reshape(TOKENS, 2, D)
    stream = cotangent.astype(jnp.float32) + (returned[:, 0] + returned[:, 1])
    stream = stream.astype(jnp.bfloat16)
    normed = (conv_out.astype(jnp.float32) - row_mean[:, None]) * row_rstd[:, None]
    scaled_norm = normed * ln_gain[None, :]
    norm_sig = jax.nn.sigmoid(scaled_norm)
    mixed = (scaled_norm * norm_sig).astype(jnp.bfloat16)
    mixed_grad = jnp.dot(stream, out_proj, preferred_element_type=jnp.float32)
    proj_g = jnp.dot(stream.T, mixed, preferred_element_type=jnp.float32)
    norm_grad = mixed_grad * norm_sig * (1.0 + scaled_norm * (1.0 - norm_sig)) * ln_gain[None, :]
    first_mean = jnp.mean(norm_grad, axis=1, keepdims=True)
    second_mean = jnp.mean(norm_grad * normed, axis=1, keepdims=True)
    conv_grad = row_rstd[:, None] * (norm_grad - first_mean - normed * second_mean)
    extended = jnp.concatenate([conv_grad, jnp.zeros((KERNEL - 1, CW), jnp.float32)], axis=0)
    tap_values = taps.astype(jnp.float32)
    unit_grad = jnp.zeros((TOKENS, CW), jnp.float32)
    for offset in range(KERNEL):
        lead = KERNEL - 1 - offset
        unit_grad = unit_grad + tap_values[offset][None, :] * extended[lead:lead + TOKENS]
    gate_sig = jax.nn.sigmoid(v_gate.astype(jnp.float32))
    value_g = (unit_grad * gate_sig).astype(jnp.bfloat16)
    gating_g = (unit_grad * v_value.astype(jnp.float32) * gate_sig * (1.0 - gate_sig)).astype(jnp.bfloat16)
    return (gate_g, up_g, down_g, proj_g, stream, value_g, gating_g)
```

```python
import functools

import jax
import jax.numpy as jnp
from jax import lax
from jax.experimental import pallas as pl
from jax.experimental.pallas import tpu as pltpu
from jax.sharding import PartitionSpec as P


def passed_along(value, axis, steps):
    count = lax.axis_size(axis)
    leading, last = (max(0, -steps), min(count, count - steps))
    return lax.ppermute(value, axis, [(source, source + steps) for source in range(leading, last)])


def route_targets(routes, experts, capacity):
    flat_routes = routes.reshape(-1)
    member = (flat_routes[:, None] == jnp.arange(experts, dtype=jnp.int32)[None, :]).astype(
        jnp.int32
    )
    earlier = jnp.cumsum(member, axis=0) - member
    slot_index = jnp.sum(earlier * member, axis=1)
    return flat_routes * capacity + slot_index


def contract_rows(left, right):
    return lax.dot_general(
        left, right, (((0,), (0,)), ((), ())), preferred_element_type=jnp.float32
    )


def contract_cols(left, right):
    return lax.dot_general(
        left, right, (((1,), (1,)), ((), ())), preferred_element_type=jnp.float32
    )


def plain_shards(
    moe_input,
    cotangent,
    routes,
    route_weight,
    w_gate,
    w_up,
    w_down,
    v_value,
    v_gate,
    conv_out,
    row_mean,
    row_rstd,
    ln_gain,
    taps,
    out_proj,
):
    experts = lax.axis_size("sp")
    tokens = routes.shape[0]
    capacity = 4 * tokens // experts
    total = experts * capacity
    buffer_row = route_targets(routes, experts, capacity)
    token_index = jnp.arange(2 * tokens, dtype=jnp.int32) // 2
    weights = route_weight.reshape(-1)
    width = moe_input.shape[1]
    picked = moe_input[token_index]
    weighted = (weights[:, None] * cotangent[token_index].astype(jnp.float32)).astype(jnp.bfloat16)
    rows_buf = jnp.zeros((total, width), jnp.bfloat16).at[buffer_row].set(picked)
    cotan_buf = jnp.zeros((total, width), jnp.bfloat16).at[buffer_row].set(weighted)
    rows_buf, cotan_buf = (
        rows_buf.reshape(experts, capacity, width),
        cotan_buf.reshape(experts, capacity, width),
    )
    part_rows, part_cotan = (
        lax.all_to_all(rows_buf, "sp", split_axis=0, concat_axis=0, tiled=True),
        lax.all_to_all(cotan_buf, "sp", split_axis=0, concat_axis=0, tiled=True),
    )
    arrived_rows, arrived_cotan = (
        lax.all_gather(part_rows, "tp", axis=2, tiled=True),
        lax.all_gather(part_cotan, "tp", axis=2, tiled=True),
    )
    width = arrived_rows.shape[2]
    expert_in = arrived_rows.reshape(total, width)
    expert_cot = arrived_cotan.reshape(total, width)
    gate_w = w_gate[0]
    up_w = w_up[0]
    down_w = w_down[0]
    gate_pre = contract_cols(expert_in, gate_w)
    up_pre = contract_cols(expert_in, up_w)
    gate_sig = jax.nn.sigmoid(gate_pre)
    gate_act = gate_pre * gate_sig
    hidden = (gate_act * up_pre).astype(jnp.bfloat16)
    down_g = contract_rows(hidden, expert_cot).astype(jnp.bfloat16)
    hidden_grad = contract_cols(expert_cot, down_w)
    gate_delta = (hidden_grad * up_pre * gate_sig * (1.0 + gate_pre * (1.0 - gate_sig))).astype(
        jnp.bfloat16
    )
    up_delta = (hidden_grad * gate_act).astype(jnp.bfloat16)
    gate_g = contract_rows(gate_delta, expert_in).astype(jnp.bfloat16)
    up_g = contract_rows(up_delta, expert_in).astype(jnp.bfloat16)
    partial_value = jnp.dot(gate_delta, gate_w, preferred_element_type=jnp.float32) + jnp.dot(
        up_delta, up_w, preferred_element_type=jnp.float32
    )
    row_share = lax.psum_scatter(
        partial_value.astype(jnp.bfloat16), "tp", scatter_dimension=1, tiled=True
    )
    slice_width = row_share.shape[1]
    returned = lax.all_to_all(
        row_share.reshape(experts, capacity, slice_width),
        "sp",
        split_axis=0,
        concat_axis=0,
        tiled=True,
    )
    mine = (
        returned.reshape(total, slice_width)[buffer_row]
        .astype(jnp.float32)
        .reshape(tokens, 2, slice_width)
    )
    stream = (cotangent.astype(jnp.float32) + (mine[:, 0] + mine[:, 1])).astype(jnp.bfloat16)
    full_stream = lax.all_gather(stream, "tp", axis=1, tiled=True)
    normed = (conv_out.astype(jnp.float32) - row_mean[:, None]) * row_rstd[:, None]
    scaled_norm = normed * ln_gain[None, :]
    norm_sig = jax.nn.sigmoid(scaled_norm)
    mixed = (scaled_norm * norm_sig).astype(jnp.bfloat16)
    columns = full_stream
    mixed_grad = jnp.dot(
        columns,
        lax.all_gather(out_proj, "sp", axis=0, tiled=True),
        preferred_element_type=jnp.float32,
    )
    columns = full_stream
    proj_g = lax.psum_scatter(
        contract_rows(columns, mixed).astype(jnp.bfloat16), "sp", scatter_dimension=0, tiled=True
    ).astype(jnp.float32)
    channels = out_proj.shape[1] * lax.axis_size("tp")
    norm_grad = mixed_grad * norm_sig * (1.0 + scaled_norm * (1.0 - norm_sig)) * ln_gain[None, :]
    first_sum, second_sum = lax.psum(
        (jnp.sum(norm_grad, axis=1), jnp.sum(norm_grad * normed, axis=1)), "tp"
    )
    first_mean = first_sum[:, None] / channels
    second_mean = second_sum[:, None] / channels
    conv_grad = row_rstd[:, None] * (norm_grad - first_mean - normed * second_mean)
    kernel = taps.shape[0]
    following = passed_along(conv_grad[: kernel - 1], "sp", -1)
    extended = jnp.concatenate([conv_grad, following], axis=0)
    tap_values = taps.astype(jnp.float32)
    unit_grad = jnp.zeros_like(conv_grad)
    for offset in range(kernel):
        lead = kernel - 1 - offset
        unit_grad = unit_grad + tap_values[offset][None, :] * extended[lead : lead + tokens]
    value_sig = jax.nn.sigmoid(v_gate.astype(jnp.float32))
    value_g = (unit_grad * value_sig).astype(jnp.bfloat16)
    gating_g = (unit_grad * v_value.astype(jnp.float32) * value_sig * (1.0 - value_sig)).astype(
        jnp.bfloat16
    )
    return (gate_g[None], up_g[None], down_g[None], proj_g, stream, value_g, gating_g)


VMEM = pl.BlockSpec(memory_space=pltpu.VMEM)


def remote(src, dst, send_sem, recv_sem, sp, tp):
    return pltpu.make_async_remote_copy(
        src_ref=src,
        dst_ref=dst,
        send_sem=send_sem,
        recv_sem=recv_sem,
        device_id={"sp": sp, "tp": tp},
        device_id_type=pl.DeviceIdType.MESH,
    )


def greet(peers):
    barrier = pltpu.get_barrier_semaphore()
    for sp, tp in peers:
        pl.semaphore_signal(
            barrier, inc=1, device_id={"sp": sp, "tp": tp}, device_id_type=pl.DeviceIdType.MESH
        )
    pl.semaphore_wait(barrier, len(peers))


def rows_of(ref, index, count):
    return ref.at[pl.ds(pl.multiple_of(index * count, count), count)]


class ChipGather:
    def __init__(self, own, everyone, sems, me, tp, count):
        self.own, self.everyone, self.me, self.tp, self.count = own, everyone, me, tp, count
        self.send, self.recv, self.relay, self.local = sems
        self.partner = me + 1 - 2 * (me % 2)
        self.ahead = [(me + 2 * e) % count for e in range(1, count // 2)]
        self.behind = [(me + count - 2 * e) % count for e in range(1, count // 2)]

    def block(self, index):
        return rows_of(self.everyone, index, self.own.shape[0])

    def first(self, target):
        return remote(
            self.own,
            self.block(self.me),
            self.send.at[target],
            self.recv.at[self.me],
            target,
            self.tp,
        )

    def onward(self, origin):
        return remote(
            self.block(origin),
            self.block(origin),
            self.relay.at[origin],
            self.recv.at[origin],
            self.partner,
            self.tp,
        )

    def start(self):
        pltpu.make_async_copy(self.own, self.block(self.me), self.local).start()
        for target in self.ahead + [self.partner]:
            self.first(target).start()

    def pass_on(self):
        for origin in self.behind:
            self.onward(origin).wait_recv()
            self.onward(origin).start()

    def finish(self):
        pltpu.make_async_copy(self.own, self.block(self.me), self.local).wait()
        for step in range(self.count // 2):
            origin = (self.partner + 2 * step) % self.count
            self.onward(origin).wait_recv()
        for target in self.ahead + [self.partner]:
            self.first(target).wait_send()
        for origin in self.behind:
            self.onward(origin).wait_send()


def gather_sems(count):
    return [
        pltpu.SemaphoreType.DMA((count,)),
        pltpu.SemaphoreType.DMA((count,)),
        pltpu.SemaphoreType.DMA((count,)),
        pltpu.SemaphoreType.DMA,
    ]


def dispatch_kernel(
    count, rows, cot, mixed, rows_out, cot_out, mixed_out, send, recv, local, *mixed_sems
):
    me, tp = lax.axis_index("sp"), lax.axis_index("tp")
    capacity, width = rows.shape[1:]
    across, down, corner = tp + 1 - 2 * (tp % 2), (tp + 2) % 4, 3 - tp
    others = [(me + d) % count for d in range(1, count)]
    greet([(other, tp) for other in others] + [(me, across), (me, down)])
    arrays = ((rows, rows_out), (cot, cot_out))

    def block(a, source, owner):
        return arrays[a][1].at[
            pl.ds(pl.multiple_of(source * capacity, capacity), capacity),
            pl.ds(pl.multiple_of(owner * width, 128), width),
        ]

    def own_copy(a):
        return pltpu.make_async_copy(arrays[a][0].at[me], block(a, me, tp), local.at[a])

    def out_copy(a, target):
        return remote(
            arrays[a][0].at[target],
            block(a, me, tp),
            send.at[a, target, 0],
            recv.at[a, me, tp],
            target,
            tp,
        )

    def side_copy(a, source, owner, target, lane):
        spot = block(a, source, owner)
        return remote(spot, spot, send.at[a, source, lane], recv.at[a, source, owner], me, target)

    for a in range(2):
        own_copy(a).start()
    for target in others:
        for a in range(2):
            out_copy(a, target).start()
    gather = ChipGather(mixed, mixed_out, mixed_sems, me, tp, count)
    gather.start()

    def relay_of(step):
        return (across, down) if step % 2 == 0 else (down, across)

    def relay(step):
        source = (me + count - step) % count
        owner, target = relay_of(step)
        for a in range(2):
            side_copy(a, source, owner, target, 3).wait_recv()
            side_copy(a, source, owner, target, 3).start()

    for step in range(count):
        source = (me + count - step) % count
        for a in range(2):
            if step == 0:
                own_copy(a).wait()
            else:
                side_copy(a, source, tp, across, 1).wait_recv()
            side_copy(a, source, tp, across, 1).start()
            side_copy(a, source, tp, down, 2).start()
        if step >= 1:
            relay(step - 1)
    relay(count - 1)
    gather.pass_on()
    for step in range(count):
        source = (me + count - step) % count
        owner, target = relay_of(step)
        for a in range(2):
            side_copy(a, source, target, across, 1).wait_recv()
            side_copy(a, source, corner, across, 1).wait_recv()
            side_copy(a, source, tp, across, 1).wait_send()
            side_copy(a, source, tp, down, 2).wait_send()
            side_copy(a, source, owner, target, 3).wait_send()
    for target in others:
        for a in range(2):
            out_copy(a, target).wait_send()
    gather.finish()


def dispatch(rows, cot, mixed, count):
    capacity, width = rows.shape[1:]
    full = jax.ShapeDtypeStruct((count * capacity, width * lax.axis_size("tp")), jnp.bfloat16)
    return pl.pallas_call(
        functools.partial(dispatch_kernel, count),
        out_shape=(
            full,
            full,
            jax.ShapeDtypeStruct((count * mixed.shape[0], mixed.shape[1]), mixed.dtype),
        ),
        in_specs=[VMEM] * 3,
        out_specs=(VMEM,) * 3,
        scratch_shapes=[
            pltpu.SemaphoreType.DMA((2, count, 4)),
            pltpu.SemaphoreType.DMA((2, count, 4)),
            pltpu.SemaphoreType.DMA((2,)),
        ]
        + gather_sems(count),
        compiler_params=pltpu.CompilerParams(
            collective_id=0, has_side_effects=True, vmem_limit_bytes=40 << 20
        ),
        name="dispatch",
        cost_estimate=pl.CostEstimate(
            flops=0, bytes_accessed=200 * rows.size * 2, transcendentals=0
        ),
    )(rows, cot, mixed)


def combine_kernel(
    count,
    partial_ref,
    cot,
    pick,
    proj,
    conv_out,
    row_mean,
    row_rstd,
    gain,
    taps,
    hidden,
    gate_delta,
    up_delta,
    expert_in,
    expert_cot,
    mine_out,
    unit_out,
    columns,
    grads,
    landed,
    middle,
    reduced,
    back,
    stream,
    proj_all,
    sums,
    arrived,
    extended,
    send,
    recv,
    back_send,
    back_recv,
    wide_send,
    wide_recv,
    strip_send,
    strip_recv,
    strip_local,
    sum_send,
    sum_recv,
    edge_send,
    edge_recv,
    *proj_sems,
):
    me, tp = lax.axis_index("sp"), lax.axis_index("tp")
    capacity, width = reduced.shape[1:]
    tokens, channels = conv_out.shape
    across, down, corner = tp + 1 - 2 * (tp % 2), (tp + 2) % 4, 3 - tp
    group = (across, down, corner)
    others = [(me + d) % count for d in range(1, count)]
    greet([(other, tp) for other in others] + [(me, other) for other in group])

    def share(source, owner):
        return partial_ref.at[
            pl.ds(pl.multiple_of(source * capacity, capacity), capacity),
            pl.ds(pl.multiple_of(owner * width, 128), width),
        ]

    order = others + [me]

    def sides(step):
        return (across, down) if step % 2 == 0 else (down, across)

    def share_copy(step, q):
        source, near = order[step], sides(step)[0]
        return remote(
            share(source, corner if q == 1 else near),
            landed.at[q, source],
            send.at[source, q],
            recv.at[source, q],
            me,
            near,
        )

    def middle_copy(step):
        source = order[step]
        return remote(
            middle.at[source],
            landed.at[2, source],
            send.at[source, 2],
            recv.at[source, 2],
            me,
            sides(step)[1],
        )

    def back_copy(target):
        return remote(
            reduced.at[target],
            rows_of(back, me, capacity),
            back_send.at[target],
            back_recv.at[me],
            target,
            tp,
        )

    def begin(step):
        for q in (1, 0):
            share_copy(step, q).start()

    def forward(step):
        source = order[step]
        share_copy(step, 1).wait_recv()
        own = share(source, sides(step)[1])[...].astype(jnp.float32)
        middle[source] = (own + landed[1, source].astype(jnp.float32)).astype(jnp.bfloat16)
        middle_copy(step).start()

    def settle(step):
        source = order[step]
        share_copy(step, 0).wait_recv()
        middle_copy(step).wait_recv()
        total = share(source, tp)[...].astype(jnp.float32)
        total = total + landed[0, source].astype(jnp.float32)
        total = (total + landed[2, source].astype(jnp.float32)).astype(jnp.bfloat16)
        if step < count - 1:
            reduced[source] = total
            back_copy(source).start()
        else:
            back[pl.ds(pl.multiple_of(me * capacity, capacity), capacity), :] = total

    products = ((gate_delta, expert_in), (up_delta, expert_in), (hidden, expert_cot))
    piece = PIECE if width % PIECE == 0 else width

    def product(spot, carry):
        spots = pl.ds(pl.multiple_of(spot * piece, 128), piece)
        for a, (left, right) in enumerate(products):
            value = jnp.dot(left[...], right[:, spots], preferred_element_type=jnp.float32)
            grads[a, :, spots] = value.astype(jnp.bfloat16)
        return carry

    pieces = 4 * width // piece
    window = min(WINDOW, count)
    for step in range(window):
        begin(step)
    gather = ChipGather(proj, proj_all, proj_sems, me, tp, count)
    gather.start()
    rstd = jnp.broadcast_to(row_rstd[...], (tokens, tokens)).T[:, 0:1]
    mean = jnp.broadcast_to(row_mean[...], (tokens, tokens)).T[:, 0:1]
    normed = (conv_out[...].astype(jnp.float32) - mean) * rstd
    scaled = normed * gain[...]
    sig = jax.nn.sigmoid(scaled)
    slope = sig * (1.0 + scaled * (1.0 - sig)) * gain[...]
    for step in range(count):
        lax.fori_loop(pieces * step // count, pieces * (step + 1) // count, product, 0)
        forward(step)
        if step + window < count:
            begin(step + window)
        if step >= 1:
            settle(step - 1)
    settle(count - 1)
    gather.pass_on()
    for other in others:
        remote(
            reduced.at[other],
            rows_of(back, other, capacity),
            back_send.at[other],
            back_recv.at[other],
            other,
            tp,
        ).wait_recv()
    mine = jnp.dot(pick[...], back[...], preferred_element_type=jnp.float32)
    mine_out[...] = mine

    def quarter(index):
        return pl.ds(pl.multiple_of(index * width, 128), width)

    stream[:, quarter(tp)] = (cot[...].astype(jnp.float32) + mine).astype(jnp.bfloat16)

    def wide_copy(q):
        spot = stream.at[:, quarter(tp)]
        return remote(spot, spot, wide_send.at[q], wide_recv.at[q], me, group[q])

    for q in range(3):
        wide_copy(q).start()
    gather.finish()

    def part(index):
        return jnp.dot(
            stream[:, quarter(index)],
            proj_all[quarter(index), :],
            preferred_element_type=jnp.float32,
        )

    mixed_grad = part(tp)
    for q in range(3):
        spot = stream.at[:, quarter(group[q])]
        remote(spot, spot, wide_send.at[q], wide_recv.at[q], me, group[q]).wait_recv()
        mixed_grad = mixed_grad + part(group[q])
    depth = stream.shape[1] // count

    def strip(index):
        return stream.at[:, pl.ds(pl.multiple_of(index * depth, 128), depth)]

    def strip_copy(target):
        return remote(
            strip(target),
            rows_of(columns, me, tokens),
            strip_send.at[target],
            strip_recv.at[me],
            target,
            tp,
        )

    norm_grad = mixed_grad * slope
    first = jnp.sum(norm_grad, axis=1, keepdims=True)
    second = jnp.sum(norm_grad * normed, axis=1, keepdims=True)
    lanes = lax.broadcasted_iota(jnp.int32, (tokens, 128), 1)
    pair = jnp.where(lanes % 2 == 0, first, second)
    sums[...] = pair.T[:8]

    def sum_copy(q):
        return remote(sums, arrived.at[q], sum_send.at[q], sum_recv.at[q], me, group[q])

    for q in range(3):
        sum_copy(q).start()
    own = pltpu.make_async_copy(strip(me), rows_of(columns, me, tokens), strip_local)
    own.start()
    for other in others:
        strip_copy(other).start()
    for q in range(3):
        sum_copy(q).wait()
    total = sums[...] + arrived[0] + arrived[1] + arrived[2]
    total = total * (1.0 / (channels * 4))
    means = jnp.concatenate([total] * 16, axis=0).T
    conv_grad = rstd * (norm_grad - means[:, 0:1] - normed * means[:, 1:2])
    extended[:tokens] = conv_grad
    halo = extended.shape[0] - tokens
    edge = remote(
        extended.at[pl.ds(0, halo)],
        extended.at[pl.ds(tokens, halo)],
        edge_send,
        edge_recv,
        (me + count - 1) % count,
        tp,
    )

    @pl.when(me > 0)
    def _():
        edge.start()

    @pl.when(me == count - 1)
    def _():
        extended[tokens:] = jnp.zeros((halo, channels), jnp.float32)

    @pl.when(me < count - 1)
    def _():
        edge.wait_recv()

    kernel = taps.shape[0]
    unit_grad = jnp.zeros((tokens, channels), jnp.float32)
    for offset in range(kernel):
        lead = kernel - 1 - offset
        tap = taps[offset : offset + 1, :].astype(jnp.float32)
        unit_grad = unit_grad + tap * extended[lead : lead + tokens, :]
    unit_out[...] = unit_grad
    own.wait()
    for other in others:
        remote(
            strip(other),
            rows_of(columns, other, tokens),
            strip_send.at[other],
            strip_recv.at[other],
            other,
            tp,
        ).wait_recv()
    for q in range(3):
        wide_copy(q).wait_send()
    for step in range(count):
        share_copy(step, 0).wait_send()
        share_copy(step, 1).wait_send()
        middle_copy(step).wait_send()
    for other in others:
        back_copy(other).wait_send()
        strip_copy(other).wait_send()

    @pl.when(me > 0)
    def _():
        edge.wait_send()


WINDOW = 3
PIECE = 256


def combine(
    partial_value, cot, pick, proj, conv_out, row_mean, row_rstd, gain, taps, acts, count
):
    tokens, width = cot.shape
    channels = conv_out.shape[1]
    capacity = partial_value.shape[0] // count
    full = partial_value.shape[1]
    depth = full // count
    halo = -(-(taps.shape[0] - 1) // 8) * 8
    dma = pltpu.SemaphoreType.DMA
    return pl.pallas_call(
        functools.partial(combine_kernel, count),
        out_shape=(
            jax.ShapeDtypeStruct((tokens, width), jnp.float32),
            jax.ShapeDtypeStruct((tokens, channels), jnp.float32),
            jax.ShapeDtypeStruct((count * tokens, depth), jnp.bfloat16),
            jax.ShapeDtypeStruct((3, acts[0].shape[0], full), jnp.bfloat16),
        ),
        in_specs=[VMEM] * 14,
        out_specs=(VMEM,) * 4,
        scratch_shapes=[
            pltpu.VMEM((3, count, capacity, width), jnp.bfloat16),
            pltpu.VMEM((count, capacity, width), jnp.bfloat16),
            pltpu.VMEM((count, capacity, width), jnp.bfloat16),
            pltpu.VMEM((count * capacity, width), jnp.bfloat16),
            pltpu.VMEM((tokens, full), jnp.bfloat16),
            pltpu.VMEM((count * proj.shape[0], proj.shape[1]), jnp.bfloat16),
            pltpu.VMEM((8, tokens), jnp.float32),
            pltpu.VMEM((3, 8, tokens), jnp.float32),
            pltpu.VMEM((tokens + halo, channels), jnp.float32),
            dma((count, 3)),
            dma((count, 3)),
            dma((count,)),
            dma((count,)),
            dma((3,)),
            dma((3,)),
            dma((count,)),
            dma((count,)),
            dma,
            dma((3,)),
            dma((3,)),
            dma,
            dma,
        ]
        + gather_sems(count),
        compiler_params=pltpu.CompilerParams(
            collective_id=1, has_side_effects=True, vmem_limit_bytes=24 << 20
        ),
        name="combine",
        cost_estimate=pl.CostEstimate(
            flops=2 * tokens * full * channels,
            bytes_accessed=50 * partial_value.size * 2,
            transcendentals=0,
        ),
    )(partial_value, cot, pick, proj, conv_out, row_mean, row_rstd, gain, taps, *acts)


def finish_kernel(
    grads,
    mine,
    unit_grad,
    columns,
    mixed,
    cot,
    v_value,
    v_gate,
    gate_out,
    up_out,
    down_out,
    proj_out,
    stream_out,
    value_out,
    gating_out,
    proj,
    stream,
    value,
    gating,
    sems,
):
    half = grads.shape[1] // 2
    copies = []
    for a, out in enumerate((gate_out, up_out, down_out)):
        for part in range(2):
            rows = pl.ds(part * half, half)
            copies.append(
                pltpu.make_async_copy(grads.at[a, rows], out.at[0, rows], sems.at[2 * a + part])
            )
    for copy in copies:
        copy.start()

    def put(local, out, index):
        copy = pltpu.make_async_copy(local, out, sems.at[index])
        copy.start()
        copies.append(copy)

    stream[...] = (cot[...].astype(jnp.float32) + mine[...]).astype(jnp.bfloat16)
    put(stream, stream_out, 6)
    unit = unit_grad[...]
    value_sig = jax.nn.sigmoid(v_gate[...].astype(jnp.float32))
    value[...] = (unit * value_sig).astype(jnp.bfloat16)
    put(value, value_out, 7)
    gating[...] = (unit * v_value[...].astype(jnp.float32) * value_sig * (1.0 - value_sig)).astype(
        jnp.bfloat16
    )
    put(gating, gating_out, 8)
    proj[...] = contract_rows(columns[...], mixed[...])
    put(proj, proj_out, 9)
    for copy in copies:
        copy.wait()


def finish(grads, mine, unit_grad, columns, mixed, cot, v_value, v_gate):
    shape = (1,) + grads.shape[1:]
    anywhere = pl.BlockSpec(memory_space=pl.ANY)
    proj_shape = (columns.shape[1], mixed.shape[1])
    return pl.pallas_call(
        finish_kernel,
        out_shape=tuple(jax.ShapeDtypeStruct(shape, jnp.bfloat16) for _ in range(3))
        + (
            jax.ShapeDtypeStruct(proj_shape, jnp.float32),
            jax.ShapeDtypeStruct(cot.shape, jnp.bfloat16),
            jax.ShapeDtypeStruct(v_value.shape, jnp.bfloat16),
            jax.ShapeDtypeStruct(v_value.shape, jnp.bfloat16),
        ),
        in_specs=[VMEM] * 8,
        out_specs=(anywhere,) * 7,
        scratch_shapes=[
            pltpu.VMEM(proj_shape, jnp.float32),
            pltpu.VMEM(cot.shape, jnp.bfloat16),
            pltpu.VMEM(v_value.shape, jnp.bfloat16),
            pltpu.VMEM(v_value.shape, jnp.bfloat16),
            pltpu.SemaphoreType.DMA((10,)),
        ],
        compiler_params=pltpu.CompilerParams(vmem_limit_bytes=24 << 20),
        name="finish",
        cost_estimate=pl.CostEstimate(
            flops=2 * columns.size * mixed.shape[1],
            bytes_accessed=2 * grads.size * 2,
            transcendentals=0,
        ),
    )(grads, mine, unit_grad, columns, mixed, cot, v_value, v_gate)


def kernel_shards(
    moe_input,
    cotangent,
    routes,
    route_weight,
    w_gate,
    w_up,
    w_down,
    v_value,
    v_gate,
    conv_out,
    row_mean,
    row_rstd,
    ln_gain,
    taps,
    out_proj,
):
    experts = lax.axis_size("sp")
    tokens, width = moe_input.shape
    capacity = 4 * tokens // experts
    total = experts * capacity
    flat_routes = routes.reshape(-1)
    member = (flat_routes[:, None] == jnp.arange(experts, dtype=jnp.int32)[None, :]).astype(
        jnp.bfloat16
    )
    index = jnp.arange(2 * tokens, dtype=jnp.int32)
    before = (index[None, :] < index[:, None]).astype(jnp.bfloat16)
    earlier = jnp.dot(before, member, preferred_element_type=jnp.float32)
    slot_index = jnp.sum(earlier * member.astype(jnp.float32), axis=1).astype(jnp.int32)
    buffer_row = (flat_routes * capacity + slot_index).reshape(tokens, 2)
    places = jnp.arange(total, dtype=jnp.int32)
    place0 = (buffer_row[:, 0][:, None] == places[None, :]).astype(jnp.bfloat16)
    place1 = (buffer_row[:, 1][:, None] == places[None, :]).astype(jnp.bfloat16)
    pick = place0 + place1
    cot32 = cotangent.astype(jnp.float32)
    weighted = jnp.concatenate(
        [
            (route_weight[:, 0:1] * cot32).astype(jnp.bfloat16),
            (route_weight[:, 1:2] * cot32).astype(jnp.bfloat16),
        ],
        axis=0,
    )
    rows_buf = contract_rows(pick, moe_input).astype(jnp.bfloat16)
    cot_buf = contract_rows(jnp.concatenate([place0, place1], axis=0), weighted).astype(
        jnp.bfloat16
    )
    normed = (conv_out.astype(jnp.float32) - row_mean[:, None]) * row_rstd[:, None]
    scaled_norm = normed * ln_gain[None, :]
    mixed = (scaled_norm * jax.nn.sigmoid(scaled_norm)).astype(jnp.bfloat16)
    expert_in, expert_cot, mixed_all = dispatch(
        rows_buf.reshape(experts, capacity, width),
        cot_buf.reshape(experts, capacity, width),
        mixed,
        experts,
    )
    gate_w = w_gate[0]
    up_w = w_up[0]
    down_w = w_down[0]
    gate_pre = contract_cols(gate_w, expert_in)
    up_pre = contract_cols(up_w, expert_in)
    gate_sig = jax.nn.sigmoid(gate_pre)
    gate_act = gate_pre * gate_sig
    hidden = (gate_act * up_pre).astype(jnp.bfloat16)
    hidden_grad = contract_cols(down_w, expert_cot)
    gate_delta = (hidden_grad * up_pre * gate_sig * (1.0 + gate_pre * (1.0 - gate_sig))).astype(
        jnp.bfloat16
    )
    up_delta = (hidden_grad * gate_act).astype(jnp.bfloat16)
    partial_value = contract_rows(gate_delta, gate_w) + contract_rows(up_delta, up_w)
    mine, unit_grad, columns, grads = combine(
        partial_value.astype(jnp.bfloat16),
        cotangent,
        pick,
        out_proj,
        conv_out,
        row_mean[None, :],
        row_rstd[None, :],
        ln_gain[None, :],
        taps,
        (hidden, gate_delta, up_delta, expert_in, expert_cot),
        experts,
    )
    return finish(grads, mine, unit_grad, columns, mixed_all, cotangent, v_value, v_gate)


def shards(*blocks):
    tokens, width = blocks[0].shape
    depth, channels = blocks[-1].shape
    experts = lax.axis_size("sp")
    square = lax.axis_size("tp") == 4 and experts % 2 == 0 and tokens == 128
    capacity = 4 * tokens // experts
    tiled = width % 128 == 0 and depth % 128 == 0 and channels % 128 == 0 and capacity % 16 == 0
    if square and tiled:
        return kernel_shards(*blocks)
    return plain_shards(*blocks)


def solution(mesh):
    return jax.shard_map(
        shards,
        mesh=mesh,
        in_specs=(
            P("sp", "tp"),
            P("sp", "tp"),
            P("sp", None),
            P("sp", None),
            P("sp", "tp", None),
            P("sp", "tp", None),
            P("sp", "tp", None),
            P("sp", "tp"),
            P("sp", "tp"),
            P("sp", "tp"),
            P("sp"),
            P("sp"),
            P("tp"),
            P(None, "tp"),
            P("sp", "tp"),
        ),
        out_specs=(
            P("sp", "tp", None),
            P("sp", "tp", None),
            P("sp", "tp", None),
            P("sp", "tp"),
            P("sp", "tp"),
            P("sp", "tp"),
            P("sp", "tp"),
        ),
        check_vma=False,
    )
```

```python
import functools

import jax
import jax.numpy as jnp
from jax import lax
from jax.experimental import pallas as pl
from jax.experimental.pallas import tpu as pltpu
from jax.sharding import PartitionSpec as P


def passed_along(value, axis, steps):
    count = lax.axis_size(axis)
    leading, last = (max(0, -steps), min(count, count - steps))
    return lax.ppermute(value, axis, [(source, source + steps) for source in range(leading, last)])


def route_targets(routes, experts, capacity):
    flat_routes = routes.reshape(-1)
    member = (flat_routes[:, None] == jnp.arange(experts, dtype=jnp.int32)[None, :]).astype(
        jnp.int32
    )
    earlier = jnp.cumsum(member, axis=0) - member
    slot_index = jnp.sum(earlier * member, axis=1)
    return flat_routes * capacity + slot_index


def contract_rows(left, right):
    return lax.dot_general(
        left, right, (((0,), (0,)), ((), ())), preferred_element_type=jnp.float32
    )


def contract_cols(left, right):
    return lax.dot_general(
        left, right, (((1,), (1,)), ((), ())), preferred_element_type=jnp.float32
    )


def plain_shards(
    moe_input,
    cotangent,
    routes,
    route_weight,
    w_gate,
    w_up,
    w_down,
    v_value,
    v_gate,
    conv_out,
    row_mean,
    row_rstd,
    ln_gain,
    taps,
    out_proj,
):
    experts = lax.axis_size("sp")
    tokens = routes.shape[0]
    capacity = 4 * tokens // experts
    total = experts * capacity
    buffer_row = route_targets(routes, experts, capacity)
    token_index = jnp.arange(2 * tokens, dtype=jnp.int32) // 2
    weights = route_weight.reshape(-1)
    width = moe_input.shape[1]
    picked = moe_input[token_index]
    weighted = (weights[:, None] * cotangent[token_index].astype(jnp.float32)).astype(jnp.bfloat16)
    rows_buf = jnp.zeros((total, width), jnp.bfloat16).at[buffer_row].set(picked)
    cotan_buf = jnp.zeros((total, width), jnp.bfloat16).at[buffer_row].set(weighted)
    rows_buf, cotan_buf = (
        rows_buf.reshape(experts, capacity, width),
        cotan_buf.reshape(experts, capacity, width),
    )
    part_rows, part_cotan = (
        lax.all_to_all(rows_buf, "sp", split_axis=0, concat_axis=0, tiled=True),
        lax.all_to_all(cotan_buf, "sp", split_axis=0, concat_axis=0, tiled=True),
    )
    arrived_rows, arrived_cotan = (
        lax.all_gather(part_rows, "tp", axis=2, tiled=True),
        lax.all_gather(part_cotan, "tp", axis=2, tiled=True),
    )
    width = arrived_rows.shape[2]
    expert_in = arrived_rows.reshape(total, width)
    expert_cot = arrived_cotan.reshape(total, width)
    gate_w = w_gate[0]
    up_w = w_up[0]
    down_w = w_down[0]
    gate_pre = contract_cols(expert_in, gate_w)
    up_pre = contract_cols(expert_in, up_w)
    gate_sig = jax.nn.sigmoid(gate_pre)
    gate_act = gate_pre * gate_sig
    hidden = (gate_act * up_pre).astype(jnp.bfloat16)
    down_g = contract_rows(hidden, expert_cot).astype(jnp.bfloat16)
    hidden_grad = contract_cols(expert_cot, down_w)
    gate_delta = (hidden_grad * up_pre * gate_sig * (1.0 + gate_pre * (1.0 - gate_sig))).astype(
        jnp.bfloat16
    )
    up_delta = (hidden_grad * gate_act).astype(jnp.bfloat16)
    gate_g = contract_rows(gate_delta, expert_in).astype(jnp.bfloat16)
    up_g = contract_rows(up_delta, expert_in).astype(jnp.bfloat16)
    partial_value = jnp.dot(gate_delta, gate_w, preferred_element_type=jnp.float32) + jnp.dot(
        up_delta, up_w, preferred_element_type=jnp.float32
    )
    row_share = lax.psum_scatter(
        partial_value.astype(jnp.bfloat16), "tp", scatter_dimension=1, tiled=True
    )
    slice_width = row_share.shape[1]
    returned = lax.all_to_all(
        row_share.reshape(experts, capacity, slice_width),
        "sp",
        split_axis=0,
        concat_axis=0,
        tiled=True,
    )
    mine = (
        returned.reshape(total, slice_width)[buffer_row]
        .astype(jnp.float32)
        .reshape(tokens, 2, slice_width)
    )
    stream = (cotangent.astype(jnp.float32) + (mine[:, 0] + mine[:, 1])).astype(jnp.bfloat16)
    full_stream = lax.all_gather(stream, "tp", axis=1, tiled=True)
    normed = (conv_out.astype(jnp.float32) - row_mean[:, None]) * row_rstd[:, None]
    scaled_norm = normed * ln_gain[None, :]
    norm_sig = jax.nn.sigmoid(scaled_norm)
    mixed = (scaled_norm * norm_sig).astype(jnp.bfloat16)
    columns = full_stream
    mixed_grad = jnp.dot(
        columns,
        lax.all_gather(out_proj, "sp", axis=0, tiled=True),
        preferred_element_type=jnp.float32,
    )
    columns = full_stream
    proj_g = lax.psum_scatter(
        contract_rows(columns, mixed).astype(jnp.bfloat16), "sp", scatter_dimension=0, tiled=True
    ).astype(jnp.float32)
    channels = out_proj.shape[1] * lax.axis_size("tp")
    norm_grad = mixed_grad * norm_sig * (1.0 + scaled_norm * (1.0 - norm_sig)) * ln_gain[None, :]
    first_sum, second_sum = lax.psum(
        (jnp.sum(norm_grad, axis=1), jnp.sum(norm_grad * normed, axis=1)), "tp"
    )
    first_mean = first_sum[:, None] / channels
    second_mean = second_sum[:, None] / channels
    conv_grad = row_rstd[:, None] * (norm_grad - first_mean - normed * second_mean)
    kernel = taps.shape[0]
    following = passed_along(conv_grad[: kernel - 1], "sp", -1)
    extended = jnp.concatenate([conv_grad, following], axis=0)
    tap_values = taps.astype(jnp.float32)
    unit_grad = jnp.zeros_like(conv_grad)
    for offset in range(kernel):
        lead = kernel - 1 - offset
        unit_grad = unit_grad + tap_values[offset][None, :] * extended[lead : lead + tokens]
    value_sig = jax.nn.sigmoid(v_gate.astype(jnp.float32))
    value_g = (unit_grad * value_sig).astype(jnp.bfloat16)
    gating_g = (unit_grad * v_value.astype(jnp.float32) * value_sig * (1.0 - value_sig)).astype(
        jnp.bfloat16
    )
    return (gate_g[None], up_g[None], down_g[None], proj_g, stream, value_g, gating_g)


VMEM = pl.BlockSpec(memory_space=pltpu.VMEM)


def remote(src, dst, send_sem, recv_sem, sp, tp):
    return pltpu.make_async_remote_copy(
        src_ref=src,
        dst_ref=dst,
        send_sem=send_sem,
        recv_sem=recv_sem,
        device_id={"sp": sp, "tp": tp},
        device_id_type=pl.DeviceIdType.MESH,
    )


def greet(peers):
    barrier = pltpu.get_barrier_semaphore()
    for sp, tp in peers:
        pl.semaphore_signal(
            barrier, inc=1, device_id={"sp": sp, "tp": tp}, device_id_type=pl.DeviceIdType.MESH
        )
    pl.semaphore_wait(barrier, len(peers))


def rows_of(ref, index, count):
    return ref.at[pl.ds(pl.multiple_of(index * count, count), count)]


def announce(peers):
    barrier = pltpu.get_barrier_semaphore()
    for sp, tp in peers:
        pl.semaphore_signal(
            barrier, inc=1, device_id={"sp": sp, "tp": tp}, device_id_type=pl.DeviceIdType.MESH
        )


def nearby(z, chips, j):
    high = 2 * z // chips
    near = (1 - high) * z + high * (chips - 1 - z)
    both = (2 * near - j + 2 * chips) // (2 * chips)
    hop = (j + 1) // 2
    two = z - hop if j % 2 == 1 else z + hop
    one = z + (1 - 2 * high) * (j - near)
    return both * two + (1 - both) * one


def dispatch_kernel(
    count,
    x,
    cot,
    routes_far,
    weights_far,
    conv_far,
    mean_far,
    rstd_far,
    gain_far,
    proj,
    rows_out,
    cot_out,
    mixed_all,
    proj_all,
    meta,
    tok_x,
    tok_c,
    metas,
    routes,
    weights,
    conv_out,
    row_mean,
    row_rstd,
    gain,
    load,
    z_send,
    z_recv,
    side_send,
    side_recv,
    relay_send,
    relay_recv,
    push_send,
    push_recv,
    meta_send,
    meta_recv,
):
    me, tp = lax.axis_index("sp"), lax.axis_index("tp")
    tokens, width = x.shape
    capacity = rows_out.shape[0] // count
    chips = count // 2
    z, lane = me // 2, me % 2
    partner = me + 1 - 2 * lane
    across, down, corner = tp + 1 - 2 * (tp % 2), (tp + 2) % 4, 3 - tp
    others = [(me + d) % count for d in range(1, count)]
    announce([(other, tp) for other in others] + [(me, across), (me, down)])
    half = tokens // 2
    toks = (tok_x, tok_c)
    gathered = (mixed_all, proj_all)

    def columns(index):
        return pl.ds(pl.multiple_of(index * width, 128), width)

    def block(a, source, owner):
        return toks[a].at[source, :, columns(owner)]

    loads = [
        pltpu.make_async_copy(far, near, load.at[index])
        for index, (far, near) in enumerate(
            (
                (x, block(0, me, tp)),
                (cot, block(1, me, tp)),
                (routes_far, routes),
                (weights_far, weights),
                (conv_far, conv_out),
                (mean_far, row_mean),
                (rstd_far, row_rstd),
                (gain_far, gain),
                (proj, rows_of(proj_all, me, proj.shape[0])),
            )
        )
    ]
    for copy in loads:
        copy.start()
    for copy in loads:
        copy.wait()
    rstd = jnp.broadcast_to(row_rstd[...], (tokens, tokens)).T[:, 0:1]
    mean = jnp.broadcast_to(row_mean[...], (tokens, tokens)).T[:, 0:1]
    scaled = (conv_out[...].astype(jnp.float32) - mean) * rstd * gain[...]
    own_mixed = rows_of(mixed_all, me, tokens)
    own_mixed[...] = (scaled * jax.nn.sigmoid(scaled)).astype(jnp.bfloat16)
    expert = lax.broadcasted_iota(jnp.int32, (count, tokens), 0)
    first = routes[0:1, :] == expert
    second = routes[1:2, :] == expert
    named = jnp.where(first | second, 1.0, 0.0).astype(jnp.bfloat16)
    before = lax.broadcasted_iota(jnp.int32, (tokens, tokens), 0) < lax.broadcasted_iota(
        jnp.int32, (tokens, tokens), 1
    )
    before = jnp.where(before, 1.0, 0.0).astype(jnp.bfloat16)
    earlier = jnp.dot(named, before, preferred_element_type=jnp.float32)
    spot = earlier + expert.astype(jnp.float32) * capacity
    spot0 = jnp.sum(jnp.where(first, spot, 0.0), axis=0, keepdims=True)
    spot1 = jnp.sum(jnp.where(second, spot, 0.0), axis=0, keepdims=True)
    meta[...] = jnp.concatenate(
        [spot0, spot1, weights[0:1, :], weights[1:2, :], jnp.zeros((4, tokens), jnp.float32)],
        axis=0,
    )
    metas[me] = meta[...]

    def piece(a, source):
        if a < 2:
            return block(a, source, tp)
        return rows_of(gathered[a - 2], source, gathered[a - 2].shape[0] // count)

    def z_copy(a, o, target, way):
        spot = piece(a, 2 * o + lane)
        return remote(
            spot,
            spot,
            z_send.at[a, o, way],
            z_recv.at[a, o],
            2 * target + lane,
            tp,
        )

    def way_of(o):
        return (z - o + chips - 1) // chips

    def z_start(a):
        for way, bound in ((1, z < chips - 1), (0, z > 0)):

            @pl.when(bound)
            def _(way=way):
                z_copy(a, z, z + 2 * way - 1, way).start()

    def z_relay(a, o):
        way = way_of(o)
        target = z + 2 * way - 1
        z_copy(a, o, z, way).wait_recv()

        @pl.when((target >= 0) & (target <= chips - 1))
        def _():
            z_copy(a, o, target, way).start()

    def z_finish(a, j):
        o = nearby(z, chips, j)
        way = way_of(o)
        target = z + 2 * way - 1

        @pl.when((target >= 0) & (target <= chips - 1))
        def _():
            z_copy(a, o, target, way).wait_send()

    def z_drain(a):
        for way, bound in ((1, z < chips - 1), (0, z > 0)):

            @pl.when(bound)
            def _(way=way):
                z_copy(a, z, z + 2 * way - 1, way).wait_send()

    def side_copy(a, o, side):
        source = 2 * o + lane
        spot = block(a, source, tp)
        return remote(
            spot,
            spot,
            side_send.at[a, o, side],
            side_recv.at[a, o, side],
            me,
            (across, down)[side],
        )

    def relay_copy(a, o, side):
        owner, target = ((across, down), (down, across))[side]
        spot = block(a, 2 * o + lane, owner).at[pl.ds(side * half, half)]
        return remote(
            spot, spot, relay_send.at[a, o, side], relay_recv.at[a, o, side], me, target
        )

    def push_copy(a, o, q, source_lane=None):
        source = 2 * o + (lane if source_lane is None else source_lane)
        spot = (
            block(a, source, (tp, across, down)[q])
            if q < 3
            else block(a, source, corner).at[pl.ds((q - 3) * half, half)]
        )
        return remote(
            spot,
            spot,
            push_send.at[a, o, q],
            push_recv.at[a, o, q],
            partner,
            tp,
        )

    def pass_copy(a, o, source_lane=None):
        spot = piece(a, 2 * o + (lane if source_lane is None else source_lane))
        return remote(spot, spot, push_send.at[a, o, 0], push_recv.at[a, o, 0], partner, tp)

    def meta_copy(target):
        return remote(
            meta, metas.at[me], meta_send.at[target], meta_recv.at[me], target, tp
        )

    def at(k):
        j, a = k // 2, k % 2
        return a, (z if j == 0 else nearby(z, chips, j))

    blocks = 2 * chips

    def spread(k):
        a, o = at(k)
        for side in range(2):
            side_copy(a, o, side).start()
        push_copy(a, o, 0).start()

    def sides(k):
        a, o = at(k)
        for side in range(2):
            side_copy(a, o, side).wait_recv()
            relay_copy(a, o, side).start()
            push_copy(a, o, 1 + side).start()

    def corners(k):
        a, o = at(k)
        for side in (1, 0):
            relay_copy(a, o, side).wait_recv()
            push_copy(a, o, 3 + side).start()

    slots = lax.broadcasted_iota(jnp.int32, (capacity, tokens), 0).astype(jnp.float32)
    slots = slots + (me * capacity).astype(jnp.float32)

    def compact(k, source):
        a = k % 2
        info = metas[source]
        hit0 = info[0:1, :] == slots
        hit1 = info[1:2, :] == slots
        place = jnp.where(hit0 | hit1, 1.0, 0.0).astype(jnp.bfloat16)
        into = rows_of((rows_out, cot_out)[a], source, capacity)
        if a == 1:
            scale = jnp.where(hit0, info[2:3, :], 0.0) + jnp.where(hit1, info[3:4, :], 0.0)
            scale = jnp.sum(scale, axis=1, keepdims=True)
        for part in range(4):
            span = pl.ds(part * width, width)
            value = jnp.dot(
                place, toks[a][source, :, span], preferred_element_type=jnp.float32
            )
            if a == 1:
                value = value * scale
            into[:, span] = value.astype(jnp.bfloat16)

    def gather_rows(k):
        a, o = at(k)
        compact(k, 2 * o + lane)
        for q in range(5):
            push_copy(a, o, q, 1 - lane).wait_recv()
        compact(k, 2 * o + 1 - lane)

    pl.semaphore_wait(pltpu.get_barrier_semaphore(), count + 1)
    for a in range(2):
        z_start(a)
        spread(a)
    for other in others:
        meta_copy(other).start()
    ahead = 2
    for n in range(blocks + 2):
        if n == 0:
            z_relay(*at(ahead))
            ahead += 1
        if n < blocks:
            sides(n)
        if n + 2 < blocks:
            spread(n + 2)
        while ahead < min(blocks, 4 + 2 * n if n < 2 else 5 + n):
            z_relay(*at(ahead))
            ahead += 1
        if n == chips - 1:
            z_start(2)
            z_start(3)
            pass_copy(2, z).start()
            pass_copy(3, z).start()
        if chips + 1 <= n < 2 * chips:
            o = nearby(z, chips, n - chips)
            for a in (2, 3):
                z_relay(a, o)
                pass_copy(a, o).start()
        if n == 1:
            for other in others:
                remote(
                    meta, metas.at[other], meta_send.at[other], meta_recv.at[other], other, tp
                ).wait_recv()
        if 1 <= n <= blocks:
            corners(n - 1)
        if 2 <= n:
            gather_rows(n - 2)
    for other in others:
        meta_copy(other).wait_send()
    for k in range(blocks):
        a, o = at(k)
        for side in range(2):
            side_copy(a, o, side).wait_send()
            relay_copy(a, o, side).wait_send()
        for q in range(5):
            push_copy(a, o, q).wait_send()
    for a in range(4):
        z_drain(a)
        for j in range(1, chips):
            z_finish(a, j)
        if a >= 2:
            for j in range(chips):
                o = z if j == 0 else nearby(z, chips, j)
                pass_copy(a, o, 1 - lane).wait_recv()
                pass_copy(a, o).wait_send()


def dispatch(x, cot, routes, weights, conv_out, row_mean, row_rstd, gain, proj, count):
    tokens, width = x.shape
    capacity = 4 * tokens // count
    chips = count // 2
    full = width * lax.axis_size("tp")
    rows = jax.ShapeDtypeStruct((count * capacity, full), jnp.bfloat16)
    dma = pltpu.SemaphoreType.DMA
    return pl.pallas_call(
        functools.partial(dispatch_kernel, count),
        out_shape=(
            rows,
            rows,
            jax.ShapeDtypeStruct((count * tokens, conv_out.shape[1]), jnp.bfloat16),
            jax.ShapeDtypeStruct((count * proj.shape[0], proj.shape[1]), jnp.bfloat16),
            jax.ShapeDtypeStruct((8, tokens), jnp.float32),
        ),
        in_specs=[pl.BlockSpec(memory_space=pltpu.HBM)] * 9,
        out_specs=(VMEM,) * 5,
        scratch_shapes=[
            pltpu.VMEM((count, tokens, full), jnp.bfloat16),
            pltpu.VMEM((count, tokens, full), jnp.bfloat16),
            pltpu.VMEM((count, 8, tokens), jnp.float32),
        ]
        + [
            pltpu.VMEM(value.shape, value.dtype)
            for value in (routes, weights, conv_out, row_mean, row_rstd, gain)
        ]
        + [
            dma((9,)),
            dma((4, chips, 2)),
            dma((4, chips)),
            dma((2, chips, 2)),
            dma((2, chips, 2)),
            dma((2, chips, 2)),
            dma((2, chips, 2)),
            dma((4, chips, 5)),
            dma((4, chips, 5)),
            dma((count,)),
            dma((count,)),
        ],
        compiler_params=pltpu.CompilerParams(
            collective_id=0, has_side_effects=True, vmem_limit_bytes=36 << 20
        ),
        name="dispatch",
        cost_estimate=pl.CostEstimate(
            flops=8 * count * capacity * tokens * full,
            bytes_accessed=200 * count * capacity * width * 2,
            transcendentals=0,
        ),
    )(*[pltpu.with_memory_space_constraint(v, pltpu.HBM) for v in (x, cot, routes, weights, conv_out, row_mean, row_rstd, gain, proj)])


def combine_kernel(
    count,
    partial_ref,
    cot,
    meta,
    proj_all,
    conv_out,
    row_mean,
    row_rstd,
    gain,
    taps,
    hidden,
    gate_delta,
    up_delta,
    expert_in,
    expert_cot,
    mine_out,
    unit_out,
    columns,
    grads,
    landed,
    middle,
    reduced,
    back,
    stream,
    sums,
    arrived,
    extended,
    send,
    recv,
    back_send,
    back_recv,
    wide_send,
    wide_recv,
    strip_send,
    strip_recv,
    strip_local,
    sum_send,
    sum_recv,
    edge_send,
    edge_recv,
):
    me, tp = lax.axis_index("sp"), lax.axis_index("tp")
    capacity, width = reduced.shape[1:]
    tokens, channels = conv_out.shape
    across, down, corner = tp + 1 - 2 * (tp % 2), (tp + 2) % 4, 3 - tp
    group = (across, down, corner)
    others = [(me + d) % count for d in range(1, count)]
    greet([(other, tp) for other in others] + [(me, other) for other in group])

    def share(source, owner):
        return partial_ref.at[
            pl.ds(pl.multiple_of(source * capacity, capacity), capacity),
            pl.ds(pl.multiple_of(owner * width, 128), width),
        ]

    order = others + [me]

    def sides(step):
        return (across, down) if step % 2 == 0 else (down, across)

    def share_copy(step, q):
        source, near = order[step], sides(step)[0]
        return remote(
            share(source, corner if q == 1 else near),
            landed.at[q, source],
            send.at[source, q],
            recv.at[source, q],
            me,
            near,
        )

    def middle_copy(step):
        source = order[step]
        return remote(
            middle.at[source],
            landed.at[2, source],
            send.at[source, 2],
            recv.at[source, 2],
            me,
            sides(step)[1],
        )

    def back_copy(target):
        return remote(
            reduced.at[target],
            rows_of(back, me, capacity),
            back_send.at[target],
            back_recv.at[me],
            target,
            tp,
        )

    def begin(step):
        for q in (1, 0):
            share_copy(step, q).start()

    def forward(step):
        source = order[step]
        share_copy(step, 1).wait_recv()
        own = share(source, sides(step)[1])[...].astype(jnp.float32)
        middle[source] = (own + landed[1, source].astype(jnp.float32)).astype(jnp.bfloat16)
        middle_copy(step).start()

    def settle(step):
        source = order[step]
        share_copy(step, 0).wait_recv()
        middle_copy(step).wait_recv()
        total = share(source, tp)[...].astype(jnp.float32)
        total = total + landed[0, source].astype(jnp.float32)
        total = (total + landed[2, source].astype(jnp.float32)).astype(jnp.bfloat16)
        if step < count - 1:
            reduced[source] = total
            back_copy(source).start()
        else:
            back[pl.ds(pl.multiple_of(me * capacity, capacity), capacity), :] = total

    products = ((gate_delta, expert_in), (up_delta, expert_in), (hidden, expert_cot))
    piece = PIECE if width % PIECE == 0 else width

    def product(spot, carry):
        spots = pl.ds(pl.multiple_of(spot * piece, 128), piece)
        for a, (left, right) in enumerate(products):
            value = jnp.dot(left[...], right[:, spots], preferred_element_type=jnp.float32)
            grads[a, :, spots] = value.astype(jnp.bfloat16)
        return carry

    pieces = 4 * width // piece
    window = min(WINDOW, count)
    for step in range(window):
        begin(step)
    slots = lax.broadcasted_iota(jnp.int32, (count * capacity, tokens), 0).astype(jnp.float32)
    pick = jnp.where((meta[0:1, :] == slots) | (meta[1:2, :] == slots), 1.0, 0.0)
    pick = pick.astype(jnp.bfloat16)
    rstd = jnp.broadcast_to(row_rstd[...], (tokens, tokens)).T[:, 0:1]
    mean = jnp.broadcast_to(row_mean[...], (tokens, tokens)).T[:, 0:1]
    normed = (conv_out[...].astype(jnp.float32) - mean) * rstd
    scaled = normed * gain[...]
    sig = jax.nn.sigmoid(scaled)
    slope = sig * (1.0 + scaled * (1.0 - sig)) * gain[...]
    for step in range(count):
        lax.fori_loop(pieces * step // count, pieces * (step + 1) // count, product, 0)
        forward(step)
        if step + window < count:
            begin(step + window)
        if step >= 1:
            settle(step - 1)
    settle(count - 1)
    for other in others:
        remote(
            reduced.at[other],
            rows_of(back, other, capacity),
            back_send.at[other],
            back_recv.at[other],
            other,
            tp,
        ).wait_recv()
    mine = contract_rows(pick, back[...])
    mine_out[...] = mine

    def quarter(index):
        return pl.ds(pl.multiple_of(index * width, 128), width)

    stream[:, quarter(tp)] = (cot[...].astype(jnp.float32) + mine).astype(jnp.bfloat16)

    def wide_copy(q):
        spot = stream.at[:, quarter(tp)]
        return remote(spot, spot, wide_send.at[q], wide_recv.at[q], me, group[q])

    for q in range(3):
        wide_copy(q).start()

    def part(index):
        return jnp.dot(
            stream[:, quarter(index)],
            proj_all[quarter(index), :],
            preferred_element_type=jnp.float32,
        )

    mixed_grad = part(tp)
    for q in range(3):
        spot = stream.at[:, quarter(group[q])]
        remote(spot, spot, wide_send.at[q], wide_recv.at[q], me, group[q]).wait_recv()
        mixed_grad = mixed_grad + part(group[q])
    depth = stream.shape[1] // count

    def strip(index):
        return stream.at[:, pl.ds(pl.multiple_of(index * depth, 128), depth)]

    def strip_copy(target):
        return remote(
            strip(target),
            rows_of(columns, me, tokens),
            strip_send.at[target],
            strip_recv.at[me],
            target,
            tp,
        )

    norm_grad = mixed_grad * slope
    first = jnp.sum(norm_grad, axis=1, keepdims=True)
    second = jnp.sum(norm_grad * normed, axis=1, keepdims=True)
    lanes = lax.broadcasted_iota(jnp.int32, (tokens, 128), 1)
    pair = jnp.where(lanes % 2 == 0, first, second)
    sums[...] = pair.T[:8]

    def sum_copy(q):
        return remote(sums, arrived.at[q], sum_send.at[q], sum_recv.at[q], me, group[q])

    for q in range(3):
        sum_copy(q).start()
    own = pltpu.make_async_copy(strip(me), rows_of(columns, me, tokens), strip_local)
    own.start()
    for other in others:
        strip_copy(other).start()
    for q in range(3):
        sum_copy(q).wait()
    total = sums[...] + arrived[0] + arrived[1] + arrived[2]
    total = total * (1.0 / (channels * 4))
    means = jnp.concatenate([total] * 16, axis=0).T
    conv_grad = rstd * (norm_grad - means[:, 0:1] - normed * means[:, 1:2])
    extended[:tokens] = conv_grad
    halo = extended.shape[0] - tokens
    edge = remote(
        extended.at[pl.ds(0, halo)],
        extended.at[pl.ds(tokens, halo)],
        edge_send,
        edge_recv,
        (me + count - 1) % count,
        tp,
    )

    @pl.when(me > 0)
    def _():
        edge.start()

    @pl.when(me == count - 1)
    def _():
        extended[tokens:] = jnp.zeros((halo, channels), jnp.float32)

    @pl.when(me < count - 1)
    def _():
        edge.wait_recv()

    kernel = taps.shape[0]
    unit_grad = jnp.zeros((tokens, channels), jnp.float32)
    for offset in range(kernel):
        lead = kernel - 1 - offset
        tap = taps[offset : offset + 1, :].astype(jnp.float32)
        unit_grad = unit_grad + tap * extended[lead : lead + tokens, :]
    unit_out[...] = unit_grad
    own.wait()
    for other in others:
        remote(
            strip(other),
            rows_of(columns, other, tokens),
            strip_send.at[other],
            strip_recv.at[other],
            other,
            tp,
        ).wait_recv()
    for q in range(3):
        wide_copy(q).wait_send()
    for step in range(count):
        share_copy(step, 0).wait_send()
        share_copy(step, 1).wait_send()
        middle_copy(step).wait_send()
    for other in others:
        back_copy(other).wait_send()
        strip_copy(other).wait_send()

    @pl.when(me > 0)
    def _():
        edge.wait_send()


WINDOW = 3
PIECE = 256


def combine(
    partial_value, cot, meta, proj, conv_out, row_mean, row_rstd, gain, taps, acts, count
):
    tokens, width = cot.shape
    channels = conv_out.shape[1]
    capacity = partial_value.shape[0] // count
    full = partial_value.shape[1]
    depth = full // count
    halo = -(-(taps.shape[0] - 1) // 8) * 8
    dma = pltpu.SemaphoreType.DMA
    return pl.pallas_call(
        functools.partial(combine_kernel, count),
        out_shape=(
            jax.ShapeDtypeStruct((tokens, width), jnp.float32),
            jax.ShapeDtypeStruct((tokens, channels), jnp.float32),
            jax.ShapeDtypeStruct((count * tokens, depth), jnp.bfloat16),
            jax.ShapeDtypeStruct((3, acts[0].shape[0], full), jnp.bfloat16),
        ),
        in_specs=[VMEM] * 14,
        out_specs=(VMEM,) * 4,
        scratch_shapes=[
            pltpu.VMEM((3, count, capacity, width), jnp.bfloat16),
            pltpu.VMEM((count, capacity, width), jnp.bfloat16),
            pltpu.VMEM((count, capacity, width), jnp.bfloat16),
            pltpu.VMEM((count * capacity, width), jnp.bfloat16),
            pltpu.VMEM((tokens, full), jnp.bfloat16),
            pltpu.VMEM((8, tokens), jnp.float32),
            pltpu.VMEM((3, 8, tokens), jnp.float32),
            pltpu.VMEM((tokens + halo, channels), jnp.float32),
            dma((count, 3)),
            dma((count, 3)),
            dma((count,)),
            dma((count,)),
            dma((3,)),
            dma((3,)),
            dma((count,)),
            dma((count,)),
            dma,
            dma((3,)),
            dma((3,)),
            dma,
            dma,
        ],
        compiler_params=pltpu.CompilerParams(
            collective_id=1, has_side_effects=True, vmem_limit_bytes=24 << 20
        ),
        name="combine",
        cost_estimate=pl.CostEstimate(
            flops=2 * tokens * full * channels,
            bytes_accessed=50 * partial_value.size * 2,
            transcendentals=0,
        ),
    )(partial_value, cot, meta, proj, conv_out, row_mean, row_rstd, gain, taps, *acts)


def finish_kernel(
    grads,
    mine,
    unit_grad,
    columns,
    mixed,
    cot,
    v_value,
    v_gate,
    gate_out,
    up_out,
    down_out,
    proj_out,
    stream_out,
    value_out,
    gating_out,
    proj,
    stream,
    value,
    gating,
    sems,
):
    half = grads.shape[1] // 2
    copies = []
    for a, out in enumerate((gate_out, up_out, down_out)):
        for part in range(2):
            rows = pl.ds(part * half, half)
            copies.append(
                pltpu.make_async_copy(grads.at[a, rows], out.at[0, rows], sems.at[2 * a + part])
            )
    for copy in copies:
        copy.start()

    def put(local, out, index):
        copy = pltpu.make_async_copy(local, out, sems.at[index])
        copy.start()
        copies.append(copy)

    stream[...] = (cot[...].astype(jnp.float32) + mine[...]).astype(jnp.bfloat16)
    put(stream, stream_out, 6)
    unit = unit_grad[...]
    value_sig = jax.nn.sigmoid(v_gate[...].astype(jnp.float32))
    value[...] = (unit * value_sig).astype(jnp.bfloat16)
    put(value, value_out, 7)
    gating[...] = (unit * v_value[...].astype(jnp.float32) * value_sig * (1.0 - value_sig)).astype(
        jnp.bfloat16
    )
    put(gating, gating_out, 8)
    proj[...] = contract_rows(columns[...], mixed[...])
    put(proj, proj_out, 9)
    for copy in copies:
        copy.wait()


def finish(grads, mine, unit_grad, columns, mixed, cot, v_value, v_gate):
    shape = (1,) + grads.shape[1:]
    anywhere = pl.BlockSpec(memory_space=pl.ANY)
    proj_shape = (columns.shape[1], mixed.shape[1])
    return pl.pallas_call(
        finish_kernel,
        out_shape=tuple(jax.ShapeDtypeStruct(shape, jnp.bfloat16) for _ in range(3))
        + (
            jax.ShapeDtypeStruct(proj_shape, jnp.float32),
            jax.ShapeDtypeStruct(cot.shape, jnp.bfloat16),
            jax.ShapeDtypeStruct(v_value.shape, jnp.bfloat16),
            jax.ShapeDtypeStruct(v_value.shape, jnp.bfloat16),
        ),
        in_specs=[VMEM] * 8,
        out_specs=(anywhere,) * 7,
        scratch_shapes=[
            pltpu.VMEM(proj_shape, jnp.float32),
            pltpu.VMEM(cot.shape, jnp.bfloat16),
            pltpu.VMEM(v_value.shape, jnp.bfloat16),
            pltpu.VMEM(v_value.shape, jnp.bfloat16),
            pltpu.SemaphoreType.DMA((10,)),
        ],
        compiler_params=pltpu.CompilerParams(vmem_limit_bytes=24 << 20),
        name="finish",
        cost_estimate=pl.CostEstimate(
            flops=2 * columns.size * mixed.shape[1],
            bytes_accessed=2 * grads.size * 2,
            transcendentals=0,
        ),
    )(grads, mine, unit_grad, columns, mixed, cot, v_value, v_gate)


def kernel_shards(
    moe_input,
    cotangent,
    routes,
    route_weight,
    w_gate,
    w_up,
    w_down,
    v_value,
    v_gate,
    conv_out,
    row_mean,
    row_rstd,
    ln_gain,
    taps,
    out_proj,
):
    experts = lax.axis_size("sp")
    expert_in, expert_cot, mixed_all, proj_all, meta = dispatch(
        moe_input,
        cotangent,
        routes.T,
        route_weight.T,
        conv_out,
        row_mean[None, :],
        row_rstd[None, :],
        ln_gain[None, :],
        out_proj,
        experts,
    )
    gate_w = w_gate[0]
    up_w = w_up[0]
    down_w = w_down[0]
    gate_pre = contract_cols(gate_w, expert_in)
    up_pre = contract_cols(up_w, expert_in)
    gate_sig = jax.nn.sigmoid(gate_pre)
    gate_act = gate_pre * gate_sig
    hidden = (gate_act * up_pre).astype(jnp.bfloat16)
    hidden_grad = contract_cols(down_w, expert_cot)
    gate_delta = (hidden_grad * up_pre * gate_sig * (1.0 + gate_pre * (1.0 - gate_sig))).astype(
        jnp.bfloat16
    )
    up_delta = (hidden_grad * gate_act).astype(jnp.bfloat16)
    partial_value = contract_rows(gate_delta, gate_w) + contract_rows(up_delta, up_w)
    mine, unit_grad, columns, grads = combine(
        partial_value.astype(jnp.bfloat16),
        cotangent,
        meta,
        proj_all,
        conv_out,
        row_mean[None, :],
        row_rstd[None, :],
        ln_gain[None, :],
        taps,
        (hidden, gate_delta, up_delta, expert_in, expert_cot),
        experts,
    )
    return finish(grads, mine, unit_grad, columns, mixed_all, cotangent, v_value, v_gate)


def shards(*blocks):
    tokens, width = blocks[0].shape
    depth, channels = blocks[-1].shape
    experts = lax.axis_size("sp")
    square = lax.axis_size("tp") == 4 and experts % 2 == 0 and tokens == 128
    capacity = 4 * tokens // experts
    tiled = width % 128 == 0 and depth % 128 == 0 and channels % 128 == 0 and capacity % 16 == 0
    if square and tiled:
        return kernel_shards(*blocks)
    return plain_shards(*blocks)


def solution(mesh):
    return jax.shard_map(
        shards,
        mesh=mesh,
        in_specs=(
            P("sp", "tp"),
            P("sp", "tp"),
            P("sp", None),
            P("sp", None),
            P("sp", "tp", None),
            P("sp", "tp", None),
            P("sp", "tp", None),
            P("sp", "tp"),
            P("sp", "tp"),
            P("sp", "tp"),
            P("sp"),
            P("sp"),
            P("tp"),
            P(None, "tp"),
            P("sp", "tp"),
        ),
        out_specs=(
            P("sp", "tp", None),
            P("sp", "tp", None),
            P("sp", "tp", None),
            P("sp", "tp"),
            P("sp", "tp"),
            P("sp", "tp"),
            P("sp", "tp"),
        ),
        check_vma=False,
    )
```

```python
import functools

import jax
import jax.numpy as jnp
from jax import lax
from jax.experimental import pallas as pl
from jax.experimental.pallas import tpu as pltpu
from jax.sharding import PartitionSpec as P


def passed_along(value, axis, steps):
    count = lax.axis_size(axis)
    leading, last = (max(0, -steps), min(count, count - steps))
    return lax.ppermute(value, axis, [(source, source + steps) for source in range(leading, last)])


def route_targets(routes, experts, capacity):
    flat_routes = routes.reshape(-1)
    member = (flat_routes[:, None] == jnp.arange(experts, dtype=jnp.int32)[None, :]).astype(
        jnp.int32
    )
    earlier = jnp.cumsum(member, axis=0) - member
    slot_index = jnp.sum(earlier * member, axis=1)
    return flat_routes * capacity + slot_index


def contract_rows(left, right):
    return lax.dot_general(
        left, right, (((0,), (0,)), ((), ())), preferred_element_type=jnp.float32
    )


def contract_cols(left, right):
    return lax.dot_general(
        left, right, (((1,), (1,)), ((), ())), preferred_element_type=jnp.float32
    )


def plain_shards(
    moe_input,
    cotangent,
    routes,
    route_weight,
    w_gate,
    w_up,
    w_down,
    v_value,
    v_gate,
    conv_out,
    row_mean,
    row_rstd,
    ln_gain,
    taps,
    out_proj,
):
    experts = lax.axis_size("sp")
    tokens = routes.shape[0]
    capacity = 4 * tokens // experts
    total = experts * capacity
    buffer_row = route_targets(routes, experts, capacity)
    token_index = jnp.arange(2 * tokens, dtype=jnp.int32) // 2
    weights = route_weight.reshape(-1)
    width = moe_input.shape[1]
    picked = moe_input[token_index]
    weighted = (weights[:, None] * cotangent[token_index].astype(jnp.float32)).astype(jnp.bfloat16)
    rows_buf = jnp.zeros((total, width), jnp.bfloat16).at[buffer_row].set(picked)
    cotan_buf = jnp.zeros((total, width), jnp.bfloat16).at[buffer_row].set(weighted)
    rows_buf, cotan_buf = (
        rows_buf.reshape(experts, capacity, width),
        cotan_buf.reshape(experts, capacity, width),
    )
    part_rows, part_cotan = (
        lax.all_to_all(rows_buf, "sp", split_axis=0, concat_axis=0, tiled=True),
        lax.all_to_all(cotan_buf, "sp", split_axis=0, concat_axis=0, tiled=True),
    )
    arrived_rows, arrived_cotan = (
        lax.all_gather(part_rows, "tp", axis=2, tiled=True),
        lax.all_gather(part_cotan, "tp", axis=2, tiled=True),
    )
    width = arrived_rows.shape[2]
    expert_in = arrived_rows.reshape(total, width)
    expert_cot = arrived_cotan.reshape(total, width)
    gate_w = w_gate[0]
    up_w = w_up[0]
    down_w = w_down[0]
    gate_pre = contract_cols(expert_in, gate_w)
    up_pre = contract_cols(expert_in, up_w)
    gate_sig = jax.nn.sigmoid(gate_pre)
    gate_act = gate_pre * gate_sig
    hidden = (gate_act * up_pre).astype(jnp.bfloat16)
    down_g = contract_rows(hidden, expert_cot).astype(jnp.bfloat16)
    hidden_grad = contract_cols(expert_cot, down_w)
    gate_delta = (hidden_grad * up_pre * gate_sig * (1.0 + gate_pre * (1.0 - gate_sig))).astype(
        jnp.bfloat16
    )
    up_delta = (hidden_grad * gate_act).astype(jnp.bfloat16)
    gate_g = contract_rows(gate_delta, expert_in).astype(jnp.bfloat16)
    up_g = contract_rows(up_delta, expert_in).astype(jnp.bfloat16)
    partial_value = jnp.dot(gate_delta, gate_w, preferred_element_type=jnp.float32) + jnp.dot(
        up_delta, up_w, preferred_element_type=jnp.float32
    )
    row_share = lax.psum_scatter(
        partial_value.astype(jnp.bfloat16), "tp", scatter_dimension=1, tiled=True
    )
    slice_width = row_share.shape[1]
    returned = lax.all_to_all(
        row_share.reshape(experts, capacity, slice_width),
        "sp",
        split_axis=0,
        concat_axis=0,
        tiled=True,
    )
    mine = (
        returned.reshape(total, slice_width)[buffer_row]
        .astype(jnp.float32)
        .reshape(tokens, 2, slice_width)
    )
    stream = (cotangent.astype(jnp.float32) + (mine[:, 0] + mine[:, 1])).astype(jnp.bfloat16)
    full_stream = lax.all_gather(stream, "tp", axis=1, tiled=True)
    normed = (conv_out.astype(jnp.float32) - row_mean[:, None]) * row_rstd[:, None]
    scaled_norm = normed * ln_gain[None, :]
    norm_sig = jax.nn.sigmoid(scaled_norm)
    mixed = (scaled_norm * norm_sig).astype(jnp.bfloat16)
    columns = full_stream
    mixed_grad = jnp.dot(
        columns,
        lax.all_gather(out_proj, "sp", axis=0, tiled=True),
        preferred_element_type=jnp.float32,
    )
    columns = full_stream
    proj_g = lax.psum_scatter(
        contract_rows(columns, mixed).astype(jnp.bfloat16), "sp", scatter_dimension=0, tiled=True
    ).astype(jnp.float32)
    channels = out_proj.shape[1] * lax.axis_size("tp")
    norm_grad = mixed_grad * norm_sig * (1.0 + scaled_norm * (1.0 - norm_sig)) * ln_gain[None, :]
    first_sum, second_sum = lax.psum(
        (jnp.sum(norm_grad, axis=1), jnp.sum(norm_grad * normed, axis=1)), "tp"
    )
    first_mean = first_sum[:, None] / channels
    second_mean = second_sum[:, None] / channels
    conv_grad = row_rstd[:, None] * (norm_grad - first_mean - normed * second_mean)
    kernel = taps.shape[0]
    following = passed_along(conv_grad[: kernel - 1], "sp", -1)
    extended = jnp.concatenate([conv_grad, following], axis=0)
    tap_values = taps.astype(jnp.float32)
    unit_grad = jnp.zeros_like(conv_grad)
    for offset in range(kernel):
        lead = kernel - 1 - offset
        unit_grad = unit_grad + tap_values[offset][None, :] * extended[lead : lead + tokens]
    value_sig = jax.nn.sigmoid(v_gate.astype(jnp.float32))
    value_g = (unit_grad * value_sig).astype(jnp.bfloat16)
    gating_g = (unit_grad * v_value.astype(jnp.float32) * value_sig * (1.0 - value_sig)).astype(
        jnp.bfloat16
    )
    return (gate_g[None], up_g[None], down_g[None], proj_g, stream, value_g, gating_g)


VMEM = pl.BlockSpec(memory_space=pltpu.VMEM)


def remote(src, dst, send_sem, recv_sem, sp, tp):
    return pltpu.make_async_remote_copy(
        src_ref=src,
        dst_ref=dst,
        send_sem=send_sem,
        recv_sem=recv_sem,
        device_id={"sp": sp, "tp": tp},
        device_id_type=pl.DeviceIdType.MESH,
    )


def rows_of(ref, index, count):
    return ref.at[pl.ds(pl.multiple_of(index * count, count), count)]


def announce(peers):
    barrier = pltpu.get_barrier_semaphore()
    for sp, tp in peers:
        pl.semaphore_signal(
            barrier, inc=1, device_id={"sp": sp, "tp": tp}, device_id_type=pl.DeviceIdType.MESH
        )


def nearby(z, chips, j):
    high = 2 * z // chips
    near = (1 - high) * z + high * (chips - 1 - z)
    both = (2 * near - j + 2 * chips) // (2 * chips)
    hop = (j + 1) // 2
    two = z - hop if j % 2 == 1 else z + hop
    one = z + (1 - 2 * high) * (j - near)
    return both * two + (1 - both) * one


def whole_kernel(
    count,
    x,
    cot,
    routes_far,
    weights_far,
    conv_far,
    mean_far,
    rstd_far,
    gain_far,
    proj,
    taps_far,
    gate_far,
    up_far,
    down_far,
    mine_out,
    unit_out,
    strips,
    mixed_all,
    grads,
    tok_x,
    tok_c,
    metas,
    meta,
    proj_all,
    routes,
    weights,
    conv_out,
    row_mean,
    row_rstd,
    gain,
    taps,
    gate_w,
    up_w,
    down_w,
    rows,
    cots,
    hidden,
    gate_delta,
    up_delta,
    first_factor,
    second_factor,
    turned,
    partial_ref,
    landed,
    middle,
    reduced,
    back,
    stream,
    sums,
    arrived,
    extended,
    load,
    z_send,
    z_recv,
    side_send,
    side_recv,
    relay_send,
    relay_recv,
    push_send,
    push_recv,
    meta_send,
    meta_recv,
    send,
    recv,
    back_send,
    back_recv,
    wide_send,
    wide_recv,
    strip_send,
    strip_recv,
    sum_send,
    sum_recv,
    part_send,
    part_recv,
    edge_send,
    edge_recv,
):
    me, tp = lax.axis_index("sp"), lax.axis_index("tp")
    tokens, width = x.shape
    capacity = rows.shape[0] // count
    units = hidden.shape[0]
    channels = conv_out.shape[1]
    chips = count // 2
    z, lane = me // 2, me % 2
    partner = me + 1 - 2 * lane
    across, down, corner = tp + 1 - 2 * (tp % 2), (tp + 2) % 4, 3 - tp
    others = [(me + d) % count for d in range(1, count)]
    group = (across, down, corner)
    announce([(other, tp) for other in others] + [(me, other) for other in group])
    half = tokens // 2
    toks = (tok_x, tok_c)
    gathered = (mixed_all, proj_all)

    def columns(index):
        return pl.ds(pl.multiple_of(index * width, 128), width)

    def block(a, source, owner):
        return toks[a].at[source, :, columns(owner)]

    loads = [
        pltpu.make_async_copy(far, near, load.at[index])
        for index, (far, near) in enumerate(
            (
                (x, block(0, me, tp)),
                (cot, block(1, me, tp)),
                (routes_far, routes),
                (weights_far, weights),
                (conv_far, conv_out),
                (mean_far, row_mean),
                (rstd_far, row_rstd),
                (gain_far, gain),
                (proj, rows_of(proj_all, me, proj.shape[0])),
                (taps_far, taps),
                (gate_far.at[0], gate_w),
                (up_far.at[0], up_w),
                (down_far.at[0], down_w),
            )
        )
    ]
    for copy in loads:
        copy.start()
    for copy in loads[:-3]:
        copy.wait()
    rstd = jnp.broadcast_to(row_rstd[...], (tokens, tokens)).T[:, 0:1]
    mean = jnp.broadcast_to(row_mean[...], (tokens, tokens)).T[:, 0:1]
    scaled = (conv_out[...].astype(jnp.float32) - mean) * rstd * gain[...]
    own_mixed = rows_of(mixed_all, me, tokens)
    own_mixed[...] = (scaled * jax.nn.sigmoid(scaled)).astype(jnp.bfloat16)
    expert = lax.broadcasted_iota(jnp.int32, (count, tokens), 0)
    first = routes[0:1, :] == expert
    second = routes[1:2, :] == expert
    named = jnp.where(first | second, 1.0, 0.0).astype(jnp.bfloat16)
    before = lax.broadcasted_iota(jnp.int32, (tokens, tokens), 0) < lax.broadcasted_iota(
        jnp.int32, (tokens, tokens), 1
    )
    before = jnp.where(before, 1.0, 0.0).astype(jnp.bfloat16)
    earlier = jnp.dot(named, before, preferred_element_type=jnp.float32)
    spot = earlier + expert.astype(jnp.float32) * capacity
    spot0 = jnp.sum(jnp.where(first, spot, 0.0), axis=0, keepdims=True)
    spot1 = jnp.sum(jnp.where(second, spot, 0.0), axis=0, keepdims=True)
    meta[...] = jnp.concatenate(
        [spot0, spot1, weights[0:1, :], weights[1:2, :], jnp.zeros((4, tokens), jnp.float32)],
        axis=0,
    )
    metas[me] = meta[...]

    def piece(a, source):
        if a < 2:
            return block(a, source, tp)
        return rows_of(gathered[a - 2], source, gathered[a - 2].shape[0] // count)

    def z_copy(a, o, target, way):
        spot = piece(a, 2 * o + lane)
        return remote(
            spot,
            spot,
            z_send.at[a, o, way],
            z_recv.at[a, o],
            2 * target + lane,
            tp,
        )

    def way_of(o):
        return (z - o + chips - 1) // chips

    def z_start(a):
        for way, bound in ((1, z < chips - 1), (0, z > 0)):

            @pl.when(bound)
            def _(way=way):
                z_copy(a, z, z + 2 * way - 1, way).start()

    def z_relay(a, o):
        way = way_of(o)
        target = z + 2 * way - 1
        z_copy(a, o, z, way).wait_recv()

        @pl.when((target >= 0) & (target <= chips - 1))
        def _():
            z_copy(a, o, target, way).start()

    def z_finish(a, j):
        o = nearby(z, chips, j)
        way = way_of(o)
        target = z + 2 * way - 1

        @pl.when((target >= 0) & (target <= chips - 1))
        def _():
            z_copy(a, o, target, way).wait_send()

    def z_drain(a):
        for way, bound in ((1, z < chips - 1), (0, z > 0)):

            @pl.when(bound)
            def _(way=way):
                z_copy(a, z, z + 2 * way - 1, way).wait_send()

    def side_copy(a, o, side):
        source = 2 * o + lane
        spot = block(a, source, tp)
        return remote(
            spot,
            spot,
            side_send.at[a, o, side],
            side_recv.at[a, o, side],
            me,
            (across, down)[side],
        )

    def relay_copy(a, o, side):
        owner, target = ((across, down), (down, across))[side]
        spot = block(a, 2 * o + lane, owner).at[pl.ds(side * half, half)]
        return remote(
            spot, spot, relay_send.at[a, o, side], relay_recv.at[a, o, side], me, target
        )

    def push_copy(a, o, q, source_lane=None):
        source = 2 * o + (lane if source_lane is None else source_lane)
        spot = (
            block(a, source, (tp, across, down)[q])
            if q < 3
            else block(a, source, corner).at[pl.ds((q - 3) * half, half)]
        )
        return remote(
            spot,
            spot,
            push_send.at[a, o, q],
            push_recv.at[a, o, q],
            partner,
            tp,
        )

    def pass_copy(a, o, source_lane=None):
        spot = piece(a, 2 * o + (lane if source_lane is None else source_lane))
        return remote(spot, spot, push_send.at[a, o, 0], push_recv.at[a, o, 0], partner, tp)

    def meta_copy(target):
        return remote(
            meta, metas.at[me], meta_send.at[target], meta_recv.at[me], target, tp
        )

    early = list(range(chips // 2))
    late = list(range(chips // 2, chips))
    line = [(a, j) for j in early for a in range(2)] + [(a, j) for a in range(2) for j in late]
    blocks = len(line)

    def plane(j):
        return z if j == 0 else nearby(z, chips, j)

    def at(k):
        a, j = line[k]
        return a, plane(j)

    def spread(k):
        a, o = at(k)
        for side in range(2):
            side_copy(a, o, side).start()
        push_copy(a, o, 0).start()

    def sides(k):
        a, o = at(k)
        for side in range(2):
            side_copy(a, o, side).wait_recv()
            relay_copy(a, o, side).start()
            push_copy(a, o, 1 + side).start()

    def corners(k):
        a, o = at(k)
        for side in (1, 0):
            relay_copy(a, o, side).wait_recv()
            push_copy(a, o, 3 + side).start()

    slots = lax.broadcasted_iota(jnp.int32, (capacity, tokens), 0).astype(jnp.float32)
    slots = slots + (me * capacity).astype(jnp.float32)

    def compact(a, source, place_at):
        info = metas[source]
        hit0 = info[0:1, :] == slots
        hit1 = info[1:2, :] == slots
        place = jnp.where(hit0 | hit1, 1.0, 0.0).astype(jnp.bfloat16)
        into = (rows, cots)[a].at[pl.ds(place_at * capacity, capacity)]
        if a == 1:
            scale = jnp.where(hit0, info[2:3, :], 0.0) + jnp.where(hit1, info[3:4, :], 0.0)
            scale = jnp.sum(scale, axis=1, keepdims=True)
        for part in range(4):
            span = pl.ds(part * width, width)
            value = jnp.dot(
                place, toks[a][source, :, span], preferred_element_type=jnp.float32
            )
            if a == 1:
                value = value * scale
            into[:, span] = value.astype(jnp.bfloat16)

    def gather_rows(k):
        a, o = at(k)
        j = line[k][1]
        compact(a, 2 * o + lane, 2 * j)
        for q in range(5):
            push_copy(a, o, q, 1 - lane).wait_recv()
        compact(a, 2 * o + 1 - lane, 2 * j + 1)

    batch = rows.shape[0] // 2
    tiles = 1
    tile = units // tiles
    breadth = 512 if width % 512 == 0 else width
    pieces = 4 * width // breadth

    def activate(h):
        span = pl.ds(h * batch, batch)

        def step(t, carry):
            u = pl.ds(pl.multiple_of(t * tile, 16), tile)
            gate = contract_cols(gate_w[u, :], rows[span, :])
            up = contract_cols(up_w[u, :], rows[span, :])
            gate_sig = jax.nn.sigmoid(gate)
            gate_act = gate * gate_sig
            hidden[u, span] = (gate_act * up).astype(jnp.bfloat16)
            first_factor[u, :] = up * gate_sig * (1.0 + gate * (1.0 - gate_sig))
            second_factor[u, :] = gate_act
            return carry

        lax.fori_loop(0, tiles, step, 0)

    def deltas(h):
        span = pl.ds(h * batch, batch)

        def step(t, carry):
            u = pl.ds(pl.multiple_of(t * tile, 16), tile)
            hidden_grad = contract_cols(down_w[u, :], cots[span, :])
            gate_delta[u, span] = (hidden_grad * first_factor[u, :]).astype(jnp.bfloat16)
            up_delta[u, span] = (hidden_grad * second_factor[u, :]).astype(jnp.bfloat16)
            return carry

        lax.fori_loop(0, tiles, step, 0)
        turned[0] = gate_delta[:, span].T
        turned[1] = up_delta[:, span].T

    def partials(h, first_piece, last_piece):
        span = pl.ds(h * batch, batch)

        def step(t, carry):
            spots = pl.ds(pl.multiple_of(t * breadth, 128), breadth)
            value = jnp.dot(turned[0], gate_w[:, spots], preferred_element_type=jnp.float32)
            value = value + jnp.dot(
                turned[1], up_w[:, spots], preferred_element_type=jnp.float32
            )
            partial_ref[span, spots] = value.astype(jnp.bfloat16)
            return carry

        lax.fori_loop(first_piece, last_piece, step, 0)

    products = ((gate_delta, rows), (up_delta, rows), (hidden, cots))

    def product(spot, carry):
        spots = pl.ds(pl.multiple_of(spot * breadth, 128), breadth)
        for a, (left, right) in enumerate(products):
            value = jnp.dot(left[...], right[:, spots], preferred_element_type=jnp.float32)
            grads[a, :, spots] = value.astype(jnp.bfloat16)
        return carry

    def share(step, owner):
        return partial_ref.at[
            pl.ds(step * capacity, capacity),
            pl.ds(pl.multiple_of(owner * width, 128), width),
        ]

    def source_of(step):
        return 2 * plane(step // 2) + (lane if step % 2 == 0 else 1 - lane)

    def near_far(step):
        return (across, down) if step % 2 == 0 else (down, across)

    def share_copy(step, q):
        near = near_far(step)[0]
        return remote(
            share(step, corner if q == 1 else near),
            landed.at[q, step],
            send.at[step, q],
            recv.at[step, q],
            me,
            near,
        )

    def middle_copy(step):
        return remote(
            middle.at[step],
            landed.at[2, step],
            send.at[step, 2],
            recv.at[step, 2],
            me,
            near_far(step)[1],
        )

    def back_copy(step):
        target = source_of(step)
        return remote(
            reduced.at[step],
            rows_of(back, me, capacity),
            back_send.at[step],
            back_recv.at[me],
            target,
            tp,
        )

    def begin(steps):
        for q in (1, 0):
            for step in steps:
                share_copy(step, q).start()

    half_count = count // 2
    lower, upper = range(half_count), range(half_count, count)

    def forward(step):
        share_copy(step, 1).wait_recv()
        own = share(step, near_far(step)[1])[...].astype(jnp.float32)
        middle[step] = (own + landed[1, step].astype(jnp.float32)).astype(jnp.bfloat16)
        middle_copy(step).start()

    def settle(step):
        share_copy(step, 0).wait_recv()
        middle_copy(step).wait_recv()
        total = share(step, tp)[...].astype(jnp.float32)
        total = total + landed[0, step].astype(jnp.float32)
        total = (total + landed[2, step].astype(jnp.float32)).astype(jnp.bfloat16)
        if step > 0:
            reduced[step] = total
            back_copy(step).start()
        else:
            back[pl.ds(pl.multiple_of(me * capacity, capacity), capacity), :] = total

    pl.semaphore_wait(pltpu.get_barrier_semaphore(), count + 2)
    for a in range(2):
        z_start(a)
        spread(a)
    for other in others:
        meta_copy(other).start()
    ahead = 2
    for n in range(blocks + 2):
        if n == 0:
            z_relay(*at(ahead))
            ahead += 1
        if n < blocks:
            sides(n)
        if n + 2 < blocks:
            spread(n + 2)
        while ahead < min(blocks, 4 if n == 0 else 3 + 2 * n):
            z_relay(*at(ahead))
            ahead += 1
        if n == chips - 1:
            z_start(2)
            z_start(3)
            pass_copy(2, z).start()
            pass_copy(3, z).start()
        if chips + 1 <= n < 2 * chips:
            o = nearby(z, chips, n - chips)
            for a in (2, 3):
                z_relay(a, o)
                pass_copy(a, o).start()
        if n == 1:
            for other in others:
                remote(
                    meta, metas.at[other], meta_send.at[other], meta_recv.at[other], other, tp
                ).wait_recv()
        if 1 <= n <= blocks:
            corners(n - 1)
        if 2 <= n:
            gather_rows(n - 2)
        if n == chips:
            for copy in loads[-3:]:
                copy.wait()
            activate(0)
        if n == chips + 1:
            deltas(0)
        if n == chips + 2:
            partials(0, 0, pieces)
        if n == chips + chips // 2 + 1:
            activate(1)
        if n == blocks - 1:
            begin(lower)
        if n == blocks:
            forward(0)
    slots_all = lax.broadcasted_iota(jnp.int32, (count * capacity, tokens), 0)
    slots_all = slots_all.astype(jnp.float32)
    deltas(1)
    for step in lower[1:]:
        partials(1, pieces * (step - 1) // (half_count - 1), pieces * step // (half_count - 1))
        if step == half_count - 1:
            begin(upper)
        forward(step)
        settle(step - 1)
    lax.fori_loop(0, pieces // 4, product, 0)
    settle(half_count - 1)
    for step in upper:
        forward(step)
        if step == half_count + 1:
            lax.fori_loop(pieces // 4, pieces // 2, product, 0)
    pick = jnp.where((meta[0:1, :] == slots_all) | (meta[1:2, :] == slots_all), 1.0, 0.0)
    pick = pick.astype(jnp.bfloat16)
    rstd = jnp.broadcast_to(row_rstd[...], (tokens, tokens)).T[:, 0:1]
    mean = jnp.broadcast_to(row_mean[...], (tokens, tokens)).T[:, 0:1]
    normed = (conv_out[...].astype(jnp.float32) - mean) * rstd
    scaled = normed * gain[...]
    sig = jax.nn.sigmoid(scaled)
    slope = sig * (1.0 + scaled * (1.0 - sig)) * gain[...]
    for step in upper:
        settle(step)
    lax.fori_loop(pieces // 2, 3 * pieces // 4, product, 0)
    for other in others:
        meta_copy(other).wait_send()
    for k in range(blocks):
        a, o = at(k)
        for side in range(2):
            side_copy(a, o, side).wait_send()
            relay_copy(a, o, side).wait_send()
        for q in range(5):
            push_copy(a, o, q).wait_send()
    for a in range(4):
        z_drain(a)
        for j in range(1, chips):
            z_finish(a, j)
        if a >= 2:
            for j in range(chips):
                o = z if j == 0 else nearby(z, chips, j)
                pass_copy(a, o, 1 - lane).wait_recv()
                pass_copy(a, o).wait_send()
    for other in others:
        remote(
            reduced.at[0],
            rows_of(back, other, capacity),
            back_send.at[0],
            back_recv.at[other],
            other,
            tp,
        ).wait_recv()
    mine = contract_rows(pick, back[...])
    mine_out[...] = mine

    def quarter(index):
        return pl.ds(pl.multiple_of(index * width, 128), width)

    stream[:, quarter(tp)] = (block(1, me, tp)[...].astype(jnp.float32) + mine).astype(jnp.bfloat16)

    def wide_copy(q):
        spot = stream.at[:, quarter(tp)]
        return remote(spot, spot, wide_send.at[q], wide_recv.at[q], me, group[q])

    for q in range(3):
        wide_copy(q).start()
    lax.fori_loop(3 * pieces // 4, pieces, product, 0)

    def share_of(index):
        return jnp.dot(
            stream[:, quarter(index)],
            proj_all[quarter(index), :],
            preferred_element_type=jnp.float32,
        )

    depth = stream.shape[1] // count
    part_rows = tokens // 4
    part_strips = count // 4

    def part_of(source, owner):
        start = pl.multiple_of(source * tokens + owner * part_rows, part_rows)
        return strips.at[pl.ds(start, part_rows)]

    def strip_copy(target):
        return remote(
            stream.at[
                pl.ds(pl.multiple_of(tp * part_rows, part_rows), part_rows),
                pl.ds(pl.multiple_of(target * depth, 128), depth),
            ],
            part_of(me, tp),
            strip_send.at[target],
            strip_recv.at[me],
            target,
            tp,
        )

    def part_copy(source, q):
        spot = part_of(source, tp)
        return remote(
            spot, spot, part_send.at[source, q], part_recv.at[source, q], me, group[q]
        )

    def strip_out(owner):
        for index in range(part_strips):
            target = owner * part_strips + index

            @pl.when(target != me)
            def _(target=target):
                strip_copy(target).start()

    strip_out(tp)
    mixed_grad = share_of(tp)
    for q in range(3):
        spot = stream.at[:, quarter(group[q])]
        remote(spot, spot, wide_send.at[q], wide_recv.at[q], me, group[q]).wait_recv()
        strip_out(group[q])
        mixed_grad = mixed_grad + share_of(group[q])
    norm_grad = mixed_grad * slope
    first = jnp.sum(norm_grad, axis=1, keepdims=True)
    second = jnp.sum(norm_grad * normed, axis=1, keepdims=True)
    lanes = lax.broadcasted_iota(jnp.int32, (tokens, 128), 1)
    pair = jnp.where(lanes % 2 == 0, first, second)
    sums[...] = pair.T[:8]

    def sum_copy(q):
        return remote(sums, arrived.at[q], sum_send.at[q], sum_recv.at[q], me, group[q])

    for q in range(3):
        sum_copy(q).start()
    own_strip = stream[:, pl.ds(pl.multiple_of(me * depth, 128), depth)]
    rows_of(strips, me, tokens)[...] = own_strip
    for q in range(3):
        sum_copy(q).wait()
    total = sums[...] + arrived[0] + arrived[1] + arrived[2]
    total = total * (1.0 / (channels * 4))
    means = jnp.concatenate([total] * 16, axis=0).T
    conv_grad = rstd * (norm_grad - means[:, 0:1] - normed * means[:, 1:2])
    extended[:tokens] = conv_grad
    halo = extended.shape[0] - tokens
    edge = remote(
        extended.at[pl.ds(0, halo)],
        extended.at[pl.ds(tokens, halo)],
        edge_send,
        edge_recv,
        (me + count - 1) % count,
        tp,
    )

    @pl.when(me > 0)
    def _():
        edge.start()

    @pl.when(me == count - 1)
    def _():
        extended[tokens:] = jnp.zeros((halo, channels), jnp.float32)

    kernel = taps.shape[0]

    def convolve(start, size):
        unit_grad = jnp.zeros((size, channels), jnp.float32)
        for offset in range(kernel):
            lead = start + kernel - 1 - offset
            tap = taps[offset : offset + 1, :].astype(jnp.float32)
            unit_grad = unit_grad + tap * extended[lead : lead + size, :]
        unit_out[start : start + size] = unit_grad

    for other in others:
        remote(
            part_of(other, tp),
            part_of(other, tp),
            strip_send.at[other],
            strip_recv.at[other],
            other,
            tp,
        ).wait_recv()
        for q in range(3):
            part_copy(other, q).start()
    convolve(0, tokens - halo)

    @pl.when(me < count - 1)
    def _():
        edge.wait_recv()

    convolve(tokens - halo, halo)
    for other in others:
        for q in range(3):
            part_copy(other, q).wait()
    for q in range(3):
        wide_copy(q).wait_send()
    for step in range(count):
        share_copy(step, 0).wait_send()
        share_copy(step, 1).wait_send()
        middle_copy(step).wait_send()
    for step in range(1, count):
        back_copy(step).wait_send()
    for other in others:
        strip_copy(other).wait_send()

    @pl.when(me > 0)
    def _():
        edge.wait_send()


def whole(x, cot, routes, weights, conv_out, row_mean, row_rstd, gain, proj, taps, gate, up, down, count):
    tokens, width = x.shape
    channels = conv_out.shape[1]
    capacity = 4 * tokens // count
    total = count * capacity
    chips = count // 2
    full = width * lax.axis_size("tp")
    depth = full // count
    units = gate.shape[1]
    halo = -(-(taps.shape[0] - 1) // 8) * 8
    bf16, f32 = jnp.bfloat16, jnp.float32
    dma = pltpu.SemaphoreType.DMA
    operands = (x, cot, routes, weights, conv_out, row_mean, row_rstd, gain, proj, taps, gate, up, down)
    vmem = [
        ((count, tokens, full), bf16),
        ((count, tokens, full), bf16),
        ((count, 8, tokens), f32),
        ((8, tokens), f32),
        ((count * proj.shape[0], proj.shape[1]), bf16),
    ]
    vmem += [
        (value.shape, value.dtype)
        for value in (routes, weights, conv_out, row_mean, row_rstd, gain, taps)
    ]
    vmem += [
        ((units, full), bf16),
        ((units, full), bf16),
        ((units, full), bf16),
        ((total, full), bf16),
        ((total, full), bf16),
        ((units, total), bf16),
        ((units, total), bf16),
        ((units, total), bf16),
        ((units, total // 2), f32),
        ((units, total // 2), f32),
        ((2, total // 2, units), bf16),
        ((total, full), bf16),
        ((3, count, capacity, width), bf16),
        ((count, capacity, width), bf16),
        ((count, capacity, width), bf16),
        ((total, width), bf16),
        ((tokens, full), bf16),
        ((8, tokens), f32),
        ((3, 8, tokens), f32),
        ((tokens + halo, channels), f32),
    ]
    sems = [(len(operands),), (4, chips, 2), (4, chips)]
    sems += [(2, chips, 2)] * 4
    sems += [(4, chips, 5)] * 2
    sems += [(count,)] * 2
    sems += [(count, 3)] * 2
    sems += [(count,)] * 2 + [(3,)] * 2 + [(count,)] * 2 + [(3,)] * 2 + [(count, 3)] * 2
    return pl.pallas_call(
        functools.partial(whole_kernel, count),
        out_shape=(
            jax.ShapeDtypeStruct((tokens, width), f32),
            jax.ShapeDtypeStruct((tokens, channels), f32),
            jax.ShapeDtypeStruct((count * tokens, depth), bf16),
            jax.ShapeDtypeStruct((count * tokens, channels), bf16),
            jax.ShapeDtypeStruct((3, units, full), bf16),
        ),
        in_specs=[pl.BlockSpec(memory_space=pltpu.HBM)] * len(operands),
        out_specs=(VMEM,) * 5,
        scratch_shapes=[pltpu.VMEM(*entry) for entry in vmem]
        + [dma(shape) for shape in sems]
        + [dma, dma],
        compiler_params=pltpu.CompilerParams(
            collective_id=0, has_side_effects=True, vmem_limit_bytes=LIMIT << 20
        ),
        name="whole",
        cost_estimate=pl.CostEstimate(
            flops=18 * units * total * full,
            bytes_accessed=200 * total * width * 2,
            transcendentals=0,
        ),
    )(*[pltpu.with_memory_space_constraint(value, pltpu.HBM) for value in operands])


LIMIT = 40


def finish_kernel(
    grads,
    mine,
    unit_grad,
    columns,
    mixed,
    cot,
    v_value,
    v_gate,
    gate_out,
    up_out,
    down_out,
    proj_out,
    stream_out,
    value_out,
    gating_out,
    proj,
    stream,
    value,
    gating,
    sems,
):
    half = grads.shape[1] // 2
    copies = []
    for a, out in enumerate((gate_out, up_out, down_out)):
        for part in range(2):
            rows = pl.ds(part * half, half)
            copies.append(
                pltpu.make_async_copy(grads.at[a, rows], out.at[0, rows], sems.at[2 * a + part])
            )
    for copy in copies:
        copy.start()

    def put(local, out, index):
        copy = pltpu.make_async_copy(local, out, sems.at[index])
        copy.start()
        copies.append(copy)

    stream[...] = (cot[...].astype(jnp.float32) + mine[...]).astype(jnp.bfloat16)
    put(stream, stream_out, 6)
    unit = unit_grad[...]
    value_sig = jax.nn.sigmoid(v_gate[...].astype(jnp.float32))
    value[...] = (unit * value_sig).astype(jnp.bfloat16)
    put(value, value_out, 7)
    gating[...] = (unit * v_value[...].astype(jnp.float32) * value_sig * (1.0 - value_sig)).astype(
        jnp.bfloat16
    )
    put(gating, gating_out, 8)
    proj[...] = contract_rows(columns[...], mixed[...])
    put(proj, proj_out, 9)
    for copy in copies:
        copy.wait()


def finish(grads, mine, unit_grad, columns, mixed, cot, v_value, v_gate):
    shape = (1,) + grads.shape[1:]
    anywhere = pl.BlockSpec(memory_space=pl.ANY)
    proj_shape = (columns.shape[1], mixed.shape[1])
    return pl.pallas_call(
        finish_kernel,
        out_shape=tuple(jax.ShapeDtypeStruct(shape, jnp.bfloat16) for _ in range(3))
        + (
            jax.ShapeDtypeStruct(proj_shape, jnp.float32),
            jax.ShapeDtypeStruct(cot.shape, jnp.bfloat16),
            jax.ShapeDtypeStruct(v_value.shape, jnp.bfloat16),
            jax.ShapeDtypeStruct(v_value.shape, jnp.bfloat16),
        ),
        in_specs=[VMEM] * 8,
        out_specs=(anywhere,) * 7,
        scratch_shapes=[
            pltpu.VMEM(proj_shape, jnp.float32),
            pltpu.VMEM(cot.shape, jnp.bfloat16),
            pltpu.VMEM(v_value.shape, jnp.bfloat16),
            pltpu.VMEM(v_value.shape, jnp.bfloat16),
            pltpu.SemaphoreType.DMA((10,)),
        ],
        compiler_params=pltpu.CompilerParams(vmem_limit_bytes=24 << 20),
        name="finish",
        cost_estimate=pl.CostEstimate(
            flops=2 * columns.size * mixed.shape[1],
            bytes_accessed=2 * grads.size * 2,
            transcendentals=0,
        ),
    )(grads, mine, unit_grad, columns, mixed, cot, v_value, v_gate)


def kernel_shards(
    moe_input,
    cotangent,
    routes,
    route_weight,
    w_gate,
    w_up,
    w_down,
    v_value,
    v_gate,
    conv_out,
    row_mean,
    row_rstd,
    ln_gain,
    taps,
    out_proj,
):
    mine, unit_grad, columns, mixed_all, grads = whole(
        moe_input,
        cotangent,
        routes.T,
        route_weight.T,
        conv_out,
        row_mean[None, :],
        row_rstd[None, :],
        ln_gain[None, :],
        out_proj,
        taps,
        w_gate,
        w_up,
        w_down,
        lax.axis_size("sp"),
    )
    return finish(grads, mine, unit_grad, columns, mixed_all, cotangent, v_value, v_gate)


def shards(*blocks):
    tokens, width = blocks[0].shape
    depth, channels = blocks[-1].shape
    experts = lax.axis_size("sp")
    square = lax.axis_size("tp") == 4 and experts % 8 == 0 and tokens == 128
    capacity = 4 * tokens // experts
    tiled = width % 128 == 0 and depth % 128 == 0 and channels % 128 == 0 and capacity % 16 == 0
    if square and tiled:
        return kernel_shards(*blocks)
    return plain_shards(*blocks)


def solution(mesh):
    return jax.shard_map(
        shards,
        mesh=mesh,
        in_specs=(
            P("sp", "tp"),
            P("sp", "tp"),
            P("sp", None),
            P("sp", None),
            P("sp", "tp", None),
            P("sp", "tp", None),
            P("sp", "tp", None),
            P("sp", "tp"),
            P("sp", "tp"),
            P("sp", "tp"),
            P("sp"),
            P("sp"),
            P("tp"),
            P(None, "tp"),
            P("sp", "tp"),
        ),
        out_specs=(
            P("sp", "tp", None),
            P("sp", "tp", None),
            P("sp", "tp", None),
            P("sp", "tp"),
            P("sp", "tp"),
            P("sp", "tp"),
            P("sp", "tp"),
        ),
        check_vma=False,
    )
```

```python
import functools

import jax
import jax.numpy as jnp
from jax import lax
from jax.experimental import pallas as pl
from jax.experimental.pallas import tpu as pltpu
from jax.sharding import PartitionSpec as P


def passed_along(value, axis, steps):
    count = lax.axis_size(axis)
    leading, last = (max(0, -steps), min(count, count - steps))
    return lax.ppermute(value, axis, [(source, source + steps) for source in range(leading, last)])


def route_targets(routes, experts, capacity):
    flat_routes = routes.reshape(-1)
    member = (flat_routes[:, None] == jnp.arange(experts, dtype=jnp.int32)[None, :]).astype(
        jnp.int32
    )
    earlier = jnp.cumsum(member, axis=0) - member
    slot_index = jnp.sum(earlier * member, axis=1)
    return flat_routes * capacity + slot_index


def contract_rows(left, right):
    return lax.dot_general(
        left, right, (((0,), (0,)), ((), ())), preferred_element_type=jnp.float32
    )


def contract_cols(left, right):
    return lax.dot_general(
        left, right, (((1,), (1,)), ((), ())), preferred_element_type=jnp.float32
    )


def plain_shards(
    moe_input,
    cotangent,
    routes,
    route_weight,
    w_gate,
    w_up,
    w_down,
    v_value,
    v_gate,
    conv_out,
    row_mean,
    row_rstd,
    ln_gain,
    taps,
    out_proj,
):
    experts = lax.axis_size("sp")
    tokens = routes.shape[0]
    capacity = 4 * tokens // experts
    total = experts * capacity
    buffer_row = route_targets(routes, experts, capacity)
    token_index = jnp.arange(2 * tokens, dtype=jnp.int32) // 2
    weights = route_weight.reshape(-1)
    width = moe_input.shape[1]
    picked = moe_input[token_index]
    weighted = (weights[:, None] * cotangent[token_index].astype(jnp.float32)).astype(jnp.bfloat16)
    rows_buf = jnp.zeros((total, width), jnp.bfloat16).at[buffer_row].set(picked)
    cotan_buf = jnp.zeros((total, width), jnp.bfloat16).at[buffer_row].set(weighted)
    rows_buf, cotan_buf = (
        rows_buf.reshape(experts, capacity, width),
        cotan_buf.reshape(experts, capacity, width),
    )
    part_rows, part_cotan = (
        lax.all_to_all(rows_buf, "sp", split_axis=0, concat_axis=0, tiled=True),
        lax.all_to_all(cotan_buf, "sp", split_axis=0, concat_axis=0, tiled=True),
    )
    arrived_rows, arrived_cotan = (
        lax.all_gather(part_rows, "tp", axis=2, tiled=True),
        lax.all_gather(part_cotan, "tp", axis=2, tiled=True),
    )
    width = arrived_rows.shape[2]
    expert_in = arrived_rows.reshape(total, width)
    expert_cot = arrived_cotan.reshape(total, width)
    gate_w = w_gate[0]
    up_w = w_up[0]
    down_w = w_down[0]
    gate_pre = contract_cols(expert_in, gate_w)
    up_pre = contract_cols(expert_in, up_w)
    gate_sig = jax.nn.sigmoid(gate_pre)
    gate_act = gate_pre * gate_sig
    hidden = (gate_act * up_pre).astype(jnp.bfloat16)
    down_g = contract_rows(hidden, expert_cot).astype(jnp.bfloat16)
    hidden_grad = contract_cols(expert_cot, down_w)
    gate_delta = (hidden_grad * up_pre * gate_sig * (1.0 + gate_pre * (1.0 - gate_sig))).astype(
        jnp.bfloat16
    )
    up_delta = (hidden_grad * gate_act).astype(jnp.bfloat16)
    gate_g = contract_rows(gate_delta, expert_in).astype(jnp.bfloat16)
    up_g = contract_rows(up_delta, expert_in).astype(jnp.bfloat16)
    partial_value = jnp.dot(gate_delta, gate_w, preferred_element_type=jnp.float32) + jnp.dot(
        up_delta, up_w, preferred_element_type=jnp.float32
    )
    row_share = lax.psum_scatter(
        partial_value.astype(jnp.bfloat16), "tp", scatter_dimension=1, tiled=True
    )
    slice_width = row_share.shape[1]
    returned = lax.all_to_all(
        row_share.reshape(experts, capacity, slice_width),
        "sp",
        split_axis=0,
        concat_axis=0,
        tiled=True,
    )
    mine = (
        returned.reshape(total, slice_width)[buffer_row]
        .astype(jnp.float32)
        .reshape(tokens, 2, slice_width)
    )
    stream = (cotangent.astype(jnp.float32) + (mine[:, 0] + mine[:, 1])).astype(jnp.bfloat16)
    full_stream = lax.all_gather(stream, "tp", axis=1, tiled=True)
    normed = (conv_out.astype(jnp.float32) - row_mean[:, None]) * row_rstd[:, None]
    scaled_norm = normed * ln_gain[None, :]
    norm_sig = jax.nn.sigmoid(scaled_norm)
    mixed = (scaled_norm * norm_sig).astype(jnp.bfloat16)
    columns = full_stream
    mixed_grad = jnp.dot(
        columns,
        lax.all_gather(out_proj, "sp", axis=0, tiled=True),
        preferred_element_type=jnp.float32,
    )
    columns = full_stream
    proj_g = lax.psum_scatter(
        contract_rows(columns, mixed).astype(jnp.bfloat16), "sp", scatter_dimension=0, tiled=True
    ).astype(jnp.float32)
    channels = out_proj.shape[1] * lax.axis_size("tp")
    norm_grad = mixed_grad * norm_sig * (1.0 + scaled_norm * (1.0 - norm_sig)) * ln_gain[None, :]
    first_sum, second_sum = lax.psum(
        (jnp.sum(norm_grad, axis=1), jnp.sum(norm_grad * normed, axis=1)), "tp"
    )
    first_mean = first_sum[:, None] / channels
    second_mean = second_sum[:, None] / channels
    conv_grad = row_rstd[:, None] * (norm_grad - first_mean - normed * second_mean)
    kernel = taps.shape[0]
    following = passed_along(conv_grad[: kernel - 1], "sp", -1)
    extended = jnp.concatenate([conv_grad, following], axis=0)
    tap_values = taps.astype(jnp.float32)
    unit_grad = jnp.zeros_like(conv_grad)
    for offset in range(kernel):
        lead = kernel - 1 - offset
        unit_grad = unit_grad + tap_values[offset][None, :] * extended[lead : lead + tokens]
    value_sig = jax.nn.sigmoid(v_gate.astype(jnp.float32))
    value_g = (unit_grad * value_sig).astype(jnp.bfloat16)
    gating_g = (unit_grad * v_value.astype(jnp.float32) * value_sig * (1.0 - value_sig)).astype(
        jnp.bfloat16
    )
    return (gate_g[None], up_g[None], down_g[None], proj_g, stream, value_g, gating_g)


VMEM = pl.BlockSpec(memory_space=pltpu.VMEM)


def remote(src, dst, send_sem, recv_sem, sp, tp):
    return pltpu.make_async_remote_copy(
        src_ref=src,
        dst_ref=dst,
        send_sem=send_sem,
        recv_sem=recv_sem,
        device_id={"sp": sp, "tp": tp},
        device_id_type=pl.DeviceIdType.MESH,
    )


def rows_of(ref, index, count):
    return ref.at[pl.ds(pl.multiple_of(index * count, count), count)]


def announce(peers):
    barrier = pltpu.get_barrier_semaphore()
    for sp, tp in peers:
        pl.semaphore_signal(
            barrier, inc=1, device_id={"sp": sp, "tp": tp}, device_id_type=pl.DeviceIdType.MESH
        )


def nearby(z, chips, j):
    high = 2 * z // chips
    near = (1 - high) * z + high * (chips - 1 - z)
    both = (2 * near - j + 2 * chips) // (2 * chips)
    hop = (j + 1) // 2
    two = z - hop if j % 2 == 1 else z + hop
    one = z + (1 - 2 * high) * (j - near)
    return both * two + (1 - both) * one


def whole_kernel(
    count,
    x,
    cot,
    routes_far,
    weights_far,
    conv_far,
    mean_far,
    rstd_far,
    gain_far,
    proj,
    taps_far,
    gate_far,
    up_far,
    down_far,
    mine_out,
    unit_out,
    strips,
    mixed_all,
    grads,
    tok_x,
    tok_c,
    metas,
    meta,
    proj_all,
    routes,
    weights,
    conv_out,
    row_mean,
    row_rstd,
    gain,
    taps,
    gate_w,
    up_w,
    down_w,
    rows,
    cots,
    hidden,
    gate_delta,
    up_delta,
    first_factor,
    second_factor,
    turned,
    partial_ref,
    landed,
    middle,
    reduced,
    back,
    stream,
    sums,
    arrived,
    extended,
    load,
    z_send,
    z_recv,
    side_send,
    side_recv,
    relay_send,
    relay_recv,
    push_send,
    push_recv,
    meta_send,
    meta_recv,
    send,
    recv,
    back_send,
    back_recv,
    wide_send,
    wide_recv,
    strip_send,
    strip_recv,
    sum_send,
    sum_recv,
    part_send,
    part_recv,
    edge_send,
    edge_recv,
):
    me, tp = lax.axis_index("sp"), lax.axis_index("tp")
    tokens, width = x.shape
    capacity = rows.shape[0] // count
    units = hidden.shape[0]
    channels = conv_out.shape[1]
    chips = count // 2
    z, lane = me // 2, me % 2
    partner = me + 1 - 2 * lane
    across, down, corner = tp + 1 - 2 * (tp % 2), (tp + 2) % 4, 3 - tp
    others = [(me + d) % count for d in range(1, count)]
    group = (across, down, corner)
    announce([(other, tp) for other in others] + [(me, other) for other in group])
    half = tokens // 2
    toks = (tok_x, tok_c)
    gathered = (mixed_all, proj_all)

    def columns(index):
        return pl.ds(pl.multiple_of(index * width, 128), width)

    def block(a, source, owner):
        return toks[a].at[source, :, columns(owner)]

    loads = [
        pltpu.make_async_copy(far, near, load.at[index])
        for index, (far, near) in enumerate(
            (
                (x, block(0, me, tp)),
                (cot, block(1, me, tp)),
                (routes_far, routes),
                (weights_far, weights),
                (conv_far, conv_out),
                (mean_far, row_mean),
                (rstd_far, row_rstd),
                (gain_far, gain),
                (proj, rows_of(proj_all, me, proj.shape[0])),
                (taps_far, taps),
                (gate_far.at[0], gate_w),
                (up_far.at[0], up_w),
                (down_far.at[0], down_w),
            )
        )
    ]
    for copy in loads:
        copy.start()
    for copy in loads[:-3]:
        copy.wait()
    rstd = jnp.broadcast_to(row_rstd[...], (tokens, tokens)).T[:, 0:1]
    mean = jnp.broadcast_to(row_mean[...], (tokens, tokens)).T[:, 0:1]
    scaled = (conv_out[...].astype(jnp.float32) - mean) * rstd * gain[...]
    own_mixed = rows_of(mixed_all, me, tokens)
    own_mixed[...] = (scaled * jax.nn.sigmoid(scaled)).astype(jnp.bfloat16)
    expert = lax.broadcasted_iota(jnp.int32, (count, tokens), 0)
    first = routes[0:1, :] == expert
    second = routes[1:2, :] == expert
    named = jnp.where(first | second, 1.0, 0.0).astype(jnp.bfloat16)
    before = lax.broadcasted_iota(jnp.int32, (tokens, tokens), 0) < lax.broadcasted_iota(
        jnp.int32, (tokens, tokens), 1
    )
    before = jnp.where(before, 1.0, 0.0).astype(jnp.bfloat16)
    earlier = jnp.dot(named, before, preferred_element_type=jnp.float32)
    spot = earlier + expert.astype(jnp.float32) * capacity
    spot0 = jnp.sum(jnp.where(first, spot, 0.0), axis=0, keepdims=True)
    spot1 = jnp.sum(jnp.where(second, spot, 0.0), axis=0, keepdims=True)
    meta[...] = jnp.concatenate(
        [spot0, spot1, weights[0:1, :], weights[1:2, :], jnp.zeros((4, tokens), jnp.float32)],
        axis=0,
    )
    metas[me] = meta[...]

    def piece(a, source):
        if a < 2:
            return block(a, source, tp)
        return rows_of(gathered[a - 2], source, gathered[a - 2].shape[0] // count)

    def z_copy(a, o, target, way):
        spot = piece(a, 2 * o + lane)
        return remote(
            spot,
            spot,
            z_send.at[a, o, way],
            z_recv.at[a, o],
            2 * target + lane,
            tp,
        )

    def way_of(o):
        return (z - o + chips - 1) // chips

    def z_start(a):
        for way, bound in ((1, z < chips - 1), (0, z > 0)):

            @pl.when(bound)
            def _(way=way):
                z_copy(a, z, z + 2 * way - 1, way).start()

    def z_relay(a, o):
        way = way_of(o)
        target = z + 2 * way - 1
        z_copy(a, o, z, way).wait_recv()

        @pl.when((target >= 0) & (target <= chips - 1))
        def _():
            z_copy(a, o, target, way).start()

    def z_finish(a, j):
        o = nearby(z, chips, j)
        way = way_of(o)
        target = z + 2 * way - 1

        @pl.when((target >= 0) & (target <= chips - 1))
        def _():
            z_copy(a, o, target, way).wait_send()

    def z_drain(a):
        for way, bound in ((1, z < chips - 1), (0, z > 0)):

            @pl.when(bound)
            def _(way=way):
                z_copy(a, z, z + 2 * way - 1, way).wait_send()

    def side_copy(a, o, side):
        source = 2 * o + lane
        spot = block(a, source, tp)
        return remote(
            spot,
            spot,
            side_send.at[a, o, side],
            side_recv.at[a, o, side],
            me,
            (across, down)[side],
        )

    def relay_copy(a, o, side):
        owner, target = ((across, down), (down, across))[side]
        spot = block(a, 2 * o + lane, owner).at[pl.ds(side * half, half)]
        return remote(
            spot, spot, relay_send.at[a, o, side], relay_recv.at[a, o, side], me, target
        )

    def push_copy(a, o, q, source_lane=None):
        source = 2 * o + (lane if source_lane is None else source_lane)
        spot = (
            block(a, source, (tp, across, down)[q])
            if q < 3
            else block(a, source, corner).at[pl.ds((q - 3) * half, half)]
        )
        return remote(
            spot,
            spot,
            push_send.at[a, o, q],
            push_recv.at[a, o, q],
            partner,
            tp,
        )

    def pass_copy(a, o, source_lane=None):
        spot = piece(a, 2 * o + (lane if source_lane is None else source_lane))
        return remote(spot, spot, push_send.at[a, o, 0], push_recv.at[a, o, 0], partner, tp)

    def meta_copy(target):
        return remote(
            meta, metas.at[me], meta_send.at[target], meta_recv.at[me], target, tp
        )

    line = [(a, j) for j in range(chips) for a in range(2)]
    seats = list(range(1, chips)) + [0]
    blocks = len(line)

    def plane(j):
        return z if j == 0 else nearby(z, chips, j)

    def at(k):
        a, j = line[k]
        return a, plane(j)

    def spread(k):
        a, o = at(k)
        for side in range(2):
            side_copy(a, o, side).start()
        push_copy(a, o, 0).start()

    def sides(k):
        a, o = at(k)
        for side in range(2):
            side_copy(a, o, side).wait_recv()
            relay_copy(a, o, side).start()
            push_copy(a, o, 1 + side).start()

    def corners(k):
        a, o = at(k)
        for side in (1, 0):
            relay_copy(a, o, side).wait_recv()
            push_copy(a, o, 3 + side).start()

    slots = lax.broadcasted_iota(jnp.int32, (capacity, tokens), 0).astype(jnp.float32)
    slots = slots + (me * capacity).astype(jnp.float32)

    def compact(a, source, place_at):
        info = metas[source]
        hit0 = info[0:1, :] == slots
        hit1 = info[1:2, :] == slots
        place = jnp.where(hit0 | hit1, 1.0, 0.0).astype(jnp.bfloat16)
        into = (rows, cots)[a].at[pl.ds(place_at * capacity, capacity)]
        if a == 1:
            scale = jnp.where(hit0, info[2:3, :], 0.0) + jnp.where(hit1, info[3:4, :], 0.0)
            scale = jnp.sum(scale, axis=1, keepdims=True)
        for part in range(4):
            span = pl.ds(part * width, width)
            value = jnp.dot(
                place, toks[a][source, :, span], preferred_element_type=jnp.float32
            )
            if a == 1:
                value = value * scale
            into[:, span] = value.astype(jnp.bfloat16)

    def gather_rows(k):
        a, o = at(k)
        seat = 2 * seats.index(line[k][1])
        compact(a, 2 * o + lane, seat + 1)
        for q in range(5):
            push_copy(a, o, q, 1 - lane).wait_recv()
        compact(a, 2 * o + 1 - lane, seat)

    small = 2 * capacity
    lower_size = rows.shape[0] - 2 * small
    own_start = rows.shape[0] - small
    breadth = BREADTH if width % BREADTH == 0 else width
    pieces = 4 * width // breadth

    def spans(start, size):
        return pl.ds(start, size), pl.ds(start, size)

    def activate(start, size):
        span, local = spans(start, size)
        gate = contract_cols(gate_w[...], rows[span, :])
        up = contract_cols(up_w[...], rows[span, :])
        gate_sig = jax.nn.sigmoid(gate)
        gate_act = gate * gate_sig
        hidden[:, span] = (gate_act * up).astype(jnp.bfloat16)
        first_factor[:, local] = up * gate_sig * (1.0 + gate * (1.0 - gate_sig))
        second_factor[:, local] = gate_act

    def deltas(start, size):
        span, local = spans(start, size)
        hidden_grad = contract_cols(down_w[...], cots[span, :])
        for index, (delta, factor) in enumerate(
            ((gate_delta, first_factor), (up_delta, second_factor))
        ):
            value = (hidden_grad * factor[:, local]).astype(jnp.bfloat16)
            delta[:, span] = value
            turned[index, local] = value.T

    def partials(start, size, first_piece, last_piece):
        span, local = spans(start, size)

        def step(t, carry):
            spots = pl.ds(pl.multiple_of(t * breadth, 128), breadth)
            value = jnp.dot(
                turned[0, local, :], gate_w[:, spots], preferred_element_type=jnp.float32
            )
            value = value + jnp.dot(
                turned[1, local, :], up_w[:, spots], preferred_element_type=jnp.float32
            )
            partial_ref[span, spots] = value.astype(jnp.bfloat16)
            return carry

        lax.fori_loop(first_piece, last_piece, step, 0)

    products = ((gate_delta, rows), (up_delta, rows), (hidden, cots))

    def product(spot, carry):
        spots = pl.ds(pl.multiple_of(spot * breadth, 128), breadth)
        for a, (left, right) in enumerate(products):
            value = jnp.dot(left[...], right[:, spots], preferred_element_type=jnp.float32)
            grads[a, :, spots] = value.astype(jnp.bfloat16)
        return carry

    def share(step, owner):
        return partial_ref.at[
            pl.ds(step * capacity, capacity),
            pl.ds(pl.multiple_of(owner * width, 128), width),
        ]

    def source_of(step):
        return 2 * plane(seats[step // 2]) + (1 - lane if step % 2 == 0 else lane)

    def near_far(step):
        return (across, down) if step % 2 == 0 else (down, across)

    def share_copy(step, q):
        near = near_far(step)[0]
        return remote(
            share(step, corner if q == 1 else near),
            landed.at[q, step],
            send.at[step, q],
            recv.at[step, q],
            me,
            near,
        )

    def middle_copy(step):
        return remote(
            middle.at[step],
            landed.at[2, step],
            send.at[step, 2],
            recv.at[step, 2],
            me,
            near_far(step)[1],
        )

    def back_copy(step):
        target = source_of(step)
        return remote(
            reduced.at[step],
            rows_of(back, me, capacity),
            back_send.at[step],
            back_recv.at[me],
            target,
            tp,
        )

    def begin(steps):
        for q in (1, 0):
            for step in steps:
                share_copy(step, q).start()

    half_count = count - 4
    lower, upper = range(half_count), range(half_count, count)

    def forward(step):
        share_copy(step, 1).wait_recv()
        own = share(step, near_far(step)[1])[...].astype(jnp.float32)
        middle[step] = (own + landed[1, step].astype(jnp.float32)).astype(jnp.bfloat16)
        middle_copy(step).start()

    def settle(step):
        share_copy(step, 0).wait_recv()
        middle_copy(step).wait_recv()
        total = share(step, tp)[...].astype(jnp.float32)
        total = total + landed[0, step].astype(jnp.float32)
        total = (total + landed[2, step].astype(jnp.float32)).astype(jnp.bfloat16)
        if step < count - 1:
            reduced[step] = total
            back_copy(step).start()
        else:
            back[pl.ds(pl.multiple_of(me * capacity, capacity), capacity), :] = total

    pl.semaphore_wait(pltpu.get_barrier_semaphore(), count + 2)
    for a in range(2):
        z_start(a)
        spread(a)
    for other in others:
        meta_copy(other).start()
    ahead = 2
    for n in range(blocks + 2):
        if n == 0:
            z_relay(*at(ahead))
            ahead += 1
        if n < blocks:
            sides(n)
        if n + 2 < blocks:
            spread(n + 2)
        while ahead < min(blocks, 4 if n == 0 else 3 + 2 * n):
            z_relay(*at(ahead))
            ahead += 1
        if n == chips - 1:
            z_start(2)
            z_start(3)
            pass_copy(2, z).start()
            pass_copy(3, z).start()
        if chips + 1 <= n < 2 * chips:
            o = nearby(z, chips, n - chips)
            for a in (2, 3):
                z_relay(a, o)
                pass_copy(a, o).start()
        if n == 1:
            for other in others:
                remote(
                    meta, metas.at[other], meta_send.at[other], meta_recv.at[other], other, tp
                ).wait_recv()
        if 1 <= n <= blocks:
            corners(n - 1)
        if 2 <= n:
            gather_rows(n - 2)
        if n == 2:
            for copy in loads[-3:]:
                copy.wait()
            activate(own_start, small)
        if n == 3:
            deltas(own_start, small)
        if n == 4:
            partials(own_start, small, 0, pieces)
        if n == blocks - 2:
            activate(0, lower_size)
        if n == blocks - 1:
            begin(upper[-2:])
            deltas(0, lower_size)
            partials(0, lower_size, 0, pieces)
            begin(lower)
        if n == blocks:
            activate(lower_size, small)
    slots_all = lax.broadcasted_iota(jnp.int32, (count * capacity, tokens), 0)
    slots_all = slots_all.astype(jnp.float32)
    deltas(lower_size, small)
    forward(0)
    forward(1)
    settle(0)
    partials(lower_size, small, 0, pieces)
    begin(upper[:-2])
    for step in lower[2:]:
        forward(step)
        settle(step - 1)
    quart = pieces // 4
    lax.fori_loop(0, quart, product, 0)
    for step in upper:
        forward(step)
        settle(step - 1)
    pick = jnp.where((meta[0:1, :] == slots_all) | (meta[1:2, :] == slots_all), 1.0, 0.0)
    pick = pick.astype(jnp.bfloat16)
    rstd = jnp.broadcast_to(row_rstd[...], (tokens, tokens)).T[:, 0:1]
    mean = jnp.broadcast_to(row_mean[...], (tokens, tokens)).T[:, 0:1]
    normed = (conv_out[...].astype(jnp.float32) - mean) * rstd
    scaled = normed * gain[...]
    sig = jax.nn.sigmoid(scaled)
    slope = sig * (1.0 + scaled * (1.0 - sig)) * gain[...]
    settle(count - 1)
    lax.fori_loop(quart, 2 * quart, product, 0)
    for other in others:
        meta_copy(other).wait_send()
    for k in range(blocks):
        a, o = at(k)
        for side in range(2):
            side_copy(a, o, side).wait_send()
            relay_copy(a, o, side).wait_send()
        for q in range(5):
            push_copy(a, o, q).wait_send()
    for a in range(4):
        z_drain(a)
        for j in range(1, chips):
            z_finish(a, j)
        if a >= 2:
            for j in range(chips):
                o = z if j == 0 else nearby(z, chips, j)
                pass_copy(a, o, 1 - lane).wait_recv()
                pass_copy(a, o).wait_send()
    for other in others:
        remote(
            reduced.at[0],
            rows_of(back, other, capacity),
            back_send.at[0],
            back_recv.at[other],
            other,
            tp,
        ).wait_recv()
    mine = contract_rows(pick, back[...])
    mine_out[...] = mine

    def quarter(index):
        return pl.ds(pl.multiple_of(index * width, 128), width)

    stream[:, quarter(tp)] = (block(1, me, tp)[...].astype(jnp.float32) + mine).astype(jnp.bfloat16)

    def wide_copy(q):
        spot = stream.at[:, quarter(tp)]
        return remote(spot, spot, wide_send.at[q], wide_recv.at[q], me, group[q])

    for q in range(3):
        wide_copy(q).start()
    lax.fori_loop(2 * quart, pieces, product, 0)

    def share_of(index):
        return jnp.dot(
            stream[:, quarter(index)],
            proj_all[quarter(index), :],
            preferred_element_type=jnp.float32,
        )

    depth = stream.shape[1] // count
    part_rows = tokens // 4
    part_strips = count // 4

    def part_of(source, owner):
        start = pl.multiple_of(source * tokens + owner * part_rows, part_rows)
        return strips.at[pl.ds(start, part_rows)]

    def strip_copy(target):
        return remote(
            stream.at[
                pl.ds(pl.multiple_of(tp * part_rows, part_rows), part_rows),
                pl.ds(pl.multiple_of(target * depth, 128), depth),
            ],
            part_of(me, tp),
            strip_send.at[target],
            strip_recv.at[me],
            target,
            tp,
        )

    def part_copy(source, q):
        spot = part_of(source, tp)
        return remote(
            spot, spot, part_send.at[source, q], part_recv.at[source, q], me, group[q]
        )

    def strip_out(owner):
        for index in range(part_strips):
            target = owner * part_strips + index

            @pl.when(target != me)
            def _(target=target):
                strip_copy(target).start()

    strip_out(tp)
    mixed_grad = share_of(tp)
    for q in range(3):
        spot = stream.at[:, quarter(group[q])]
        remote(spot, spot, wide_send.at[q], wide_recv.at[q], me, group[q]).wait_recv()
        strip_out(group[q])
        mixed_grad = mixed_grad + share_of(group[q])
    norm_grad = mixed_grad * slope
    first = jnp.sum(norm_grad, axis=1, keepdims=True)
    second = jnp.sum(norm_grad * normed, axis=1, keepdims=True)
    lanes = lax.broadcasted_iota(jnp.int32, (tokens, 128), 1)
    pair = jnp.where(lanes % 2 == 0, first, second)
    sums[...] = pair.T[:8]

    def sum_copy(q):
        return remote(sums, arrived.at[q], sum_send.at[q], sum_recv.at[q], me, group[q])

    for q in range(3):
        sum_copy(q).start()
    own_strip = stream[:, pl.ds(pl.multiple_of(me * depth, 128), depth)]
    rows_of(strips, me, tokens)[...] = own_strip
    for q in range(3):
        sum_copy(q).wait()
    total = sums[...] + arrived[0] + arrived[1] + arrived[2]
    total = total * (1.0 / (channels * 4))
    means = jnp.concatenate([total] * 16, axis=0).T
    conv_grad = rstd * (norm_grad - means[:, 0:1] - normed * means[:, 1:2])
    extended[:tokens] = conv_grad
    halo = extended.shape[0] - tokens
    edge = remote(
        extended.at[pl.ds(0, halo)],
        extended.at[pl.ds(tokens, halo)],
        edge_send,
        edge_recv,
        (me + count - 1) % count,
        tp,
    )

    @pl.when(me > 0)
    def _():
        edge.start()

    @pl.when(me == count - 1)
    def _():
        extended[tokens:] = jnp.zeros((halo, channels), jnp.float32)

    kernel = taps.shape[0]

    def convolve(start, size):
        unit_grad = jnp.zeros((size, channels), jnp.float32)
        for offset in range(kernel):
            lead = start + kernel - 1 - offset
            tap = taps[offset : offset + 1, :].astype(jnp.float32)
            unit_grad = unit_grad + tap * extended[lead : lead + size, :]
        unit_out[start : start + size] = unit_grad

    for other in others:
        remote(
            part_of(other, tp),
            part_of(other, tp),
            strip_send.at[other],
            strip_recv.at[other],
            other,
            tp,
        ).wait_recv()
        for q in range(3):
            part_copy(other, q).start()
    convolve(0, tokens - halo)

    @pl.when(me < count - 1)
    def _():
        edge.wait_recv()

    convolve(tokens - halo, halo)
    for other in others:
        for q in range(3):
            part_copy(other, q).wait()
    for q in range(3):
        wide_copy(q).wait_send()
    for step in range(count):
        share_copy(step, 0).wait_send()
        share_copy(step, 1).wait_send()
        middle_copy(step).wait_send()
    for step in range(count - 1):
        back_copy(step).wait_send()
    for other in others:
        strip_copy(other).wait_send()

    @pl.when(me > 0)
    def _():
        edge.wait_send()


def whole(x, cot, routes, weights, conv_out, row_mean, row_rstd, gain, proj, taps, gate, up, down, count):
    tokens, width = x.shape
    channels = conv_out.shape[1]
    capacity = 4 * tokens // count
    total = count * capacity
    chips = count // 2
    full = width * lax.axis_size("tp")
    depth = full // count
    units = gate.shape[1]
    halo = -(-(taps.shape[0] - 1) // 8) * 8
    bf16, f32 = jnp.bfloat16, jnp.float32
    dma = pltpu.SemaphoreType.DMA
    operands = (x, cot, routes, weights, conv_out, row_mean, row_rstd, gain, proj, taps, gate, up, down)
    vmem = [
        ((count, tokens, full), bf16),
        ((count, tokens, full), bf16),
        ((count, 8, tokens), f32),
        ((8, tokens), f32),
        ((count * proj.shape[0], proj.shape[1]), bf16),
    ]
    vmem += [
        (value.shape, value.dtype)
        for value in (routes, weights, conv_out, row_mean, row_rstd, gain, taps)
    ]
    vmem += [
        ((units, full), bf16),
        ((units, full), bf16),
        ((units, full), bf16),
        ((total, full), bf16),
        ((total, full), bf16),
        ((units, total), bf16),
        ((units, total), bf16),
        ((units, total), bf16),
        ((units, total), f32),
        ((units, total), f32),
        ((2, total, units), bf16),
        ((total, full), bf16),
        ((3, count, capacity, width), bf16),
        ((count, capacity, width), bf16),
        ((count, capacity, width), bf16),
        ((total, width), bf16),
        ((tokens, full), bf16),
        ((8, tokens), f32),
        ((3, 8, tokens), f32),
        ((tokens + halo, channels), f32),
    ]
    sems = [(len(operands),), (4, chips, 2), (4, chips)]
    sems += [(2, chips, 2)] * 4
    sems += [(4, chips, 5)] * 2
    sems += [(count,)] * 2
    sems += [(count, 3)] * 2
    sems += [(count,)] * 2 + [(3,)] * 2 + [(count,)] * 2 + [(3,)] * 2 + [(count, 3)] * 2
    return pl.pallas_call(
        functools.partial(whole_kernel, count),
        out_shape=(
            jax.ShapeDtypeStruct((tokens, width), f32),
            jax.ShapeDtypeStruct((tokens, channels), f32),
            jax.ShapeDtypeStruct((count * tokens, depth), bf16),
            jax.ShapeDtypeStruct((count * tokens, channels), bf16),
            jax.ShapeDtypeStruct((3, units, full), bf16),
        ),
        in_specs=[pl.BlockSpec(memory_space=pltpu.HBM)] * len(operands),
        out_specs=(VMEM,) * 5,
        scratch_shapes=[pltpu.VMEM(*entry) for entry in vmem]
        + [dma(shape) for shape in sems]
        + [dma, dma],
        compiler_params=pltpu.CompilerParams(
            collective_id=0, has_side_effects=True, vmem_limit_bytes=LIMIT << 20
        ),
        name="whole",
        cost_estimate=pl.CostEstimate(
            flops=18 * units * total * full,
            bytes_accessed=200 * total * width * 2,
            transcendentals=0,
        ),
    )(*[pltpu.with_memory_space_constraint(value, pltpu.HBM) for value in operands])


LIMIT = 42
BREADTH = 512


def finish_kernel(
    grads,
    mine,
    unit_grad,
    columns,
    mixed,
    cot,
    v_value,
    v_gate,
    gate_out,
    up_out,
    down_out,
    proj_out,
    stream_out,
    value_out,
    gating_out,
    proj,
    stream,
    value,
    gating,
    sems,
):
    half = grads.shape[1] // 2
    copies = []
    for a, out in enumerate((gate_out, up_out, down_out)):
        for part in range(2):
            rows = pl.ds(part * half, half)
            copies.append(
                pltpu.make_async_copy(grads.at[a, rows], out.at[0, rows], sems.at[2 * a + part])
            )
    for copy in copies:
        copy.start()

    def put(local, out, index):
        copy = pltpu.make_async_copy(local, out, sems.at[index])
        copy.start()
        copies.append(copy)

    stream[...] = (cot[...].astype(jnp.float32) + mine[...]).astype(jnp.bfloat16)
    put(stream, stream_out, 6)
    unit = unit_grad[...]
    value_sig = jax.nn.sigmoid(v_gate[...].astype(jnp.float32))
    value[...] = (unit * value_sig).astype(jnp.bfloat16)
    put(value, value_out, 7)
    gating[...] = (unit * v_value[...].astype(jnp.float32) * value_sig * (1.0 - value_sig)).astype(
        jnp.bfloat16
    )
    put(gating, gating_out, 8)
    proj[...] = contract_rows(columns[...], mixed[...])
    put(proj, proj_out, 9)
    for copy in copies:
        copy.wait()


def finish(grads, mine, unit_grad, columns, mixed, cot, v_value, v_gate):
    shape = (1,) + grads.shape[1:]
    anywhere = pl.BlockSpec(memory_space=pl.ANY)
    proj_shape = (columns.shape[1], mixed.shape[1])
    return pl.pallas_call(
        finish_kernel,
        out_shape=tuple(jax.ShapeDtypeStruct(shape, jnp.bfloat16) for _ in range(3))
        + (
            jax.ShapeDtypeStruct(proj_shape, jnp.float32),
            jax.ShapeDtypeStruct(cot.shape, jnp.bfloat16),
            jax.ShapeDtypeStruct(v_value.shape, jnp.bfloat16),
            jax.ShapeDtypeStruct(v_value.shape, jnp.bfloat16),
        ),
        in_specs=[VMEM] * 8,
        out_specs=(anywhere,) * 7,
        scratch_shapes=[
            pltpu.VMEM(proj_shape, jnp.float32),
            pltpu.VMEM(cot.shape, jnp.bfloat16),
            pltpu.VMEM(v_value.shape, jnp.bfloat16),
            pltpu.VMEM(v_value.shape, jnp.bfloat16),
            pltpu.SemaphoreType.DMA((10,)),
        ],
        compiler_params=pltpu.CompilerParams(vmem_limit_bytes=24 << 20),
        name="finish",
        cost_estimate=pl.CostEstimate(
            flops=2 * columns.size * mixed.shape[1],
            bytes_accessed=2 * grads.size * 2,
            transcendentals=0,
        ),
    )(grads, mine, unit_grad, columns, mixed, cot, v_value, v_gate)


def kernel_shards(
    moe_input,
    cotangent,
    routes,
    route_weight,
    w_gate,
    w_up,
    w_down,
    v_value,
    v_gate,
    conv_out,
    row_mean,
    row_rstd,
    ln_gain,
    taps,
    out_proj,
):
    mine, unit_grad, columns, mixed_all, grads = whole(
        moe_input,
        cotangent,
        routes.T,
        route_weight.T,
        conv_out,
        row_mean[None, :],
        row_rstd[None, :],
        ln_gain[None, :],
        out_proj,
        taps,
        w_gate,
        w_up,
        w_down,
        lax.axis_size("sp"),
    )
    return finish(grads, mine, unit_grad, columns, mixed_all, cotangent, v_value, v_gate)


def shards(*blocks):
    tokens, width = blocks[0].shape
    depth, channels = blocks[-1].shape
    experts = lax.axis_size("sp")
    square = lax.axis_size("tp") == 4 and experts % 8 == 0 and tokens == 128
    capacity = 4 * tokens // experts
    tiled = width % 128 == 0 and depth % 128 == 0 and channels % 128 == 0 and capacity % 16 == 0
    if square and tiled:
        return kernel_shards(*blocks)
    return plain_shards(*blocks)


def solution(mesh):
    return jax.shard_map(
        shards,
        mesh=mesh,
        in_specs=(
            P("sp", "tp"),
            P("sp", "tp"),
            P("sp", None),
            P("sp", None),
            P("sp", "tp", None),
            P("sp", "tp", None),
            P("sp", "tp", None),
            P("sp", "tp"),
            P("sp", "tp"),
            P("sp", "tp"),
            P("sp"),
            P("sp"),
            P("tp"),
            P(None, "tp"),
            P("sp", "tp"),
        ),
        out_specs=(
            P("sp", "tp", None),
            P("sp", "tp", None),
            P("sp", "tp", None),
            P("sp", "tp"),
            P("sp", "tp"),
            P("sp", "tp"),
            P("sp", "tp"),
        ),
        check_vma=False,
    )
```
